32 devices in a mesh: grp: 2 (over y), sp: 4 (over z), tp: 4 (over x, core).
Axes of the slice: x: 2, y: 2, z: 4, core: 2. Of those that a mesh axis runs over, the one named last changes fastest.
Arguments:
- latents: bfloat16 [4096, 2048], P(('grp', 'sp', 'tp')), parts along dimension 0, may hold values from -6 to 6
- conv_value: bfloat16 [4096, 1024], P(('grp', 'sp'), 'tp'), parts along dimension 0, may hold values from -6 to 6
- conv_gate: bfloat16 [4096, 1024], P(('grp', 'sp'), 'tp'), parts along dimension 0, may hold values from -6 to 6
- conv_taps: float32 [31, 1024], P(None, 'tp'), may hold values from -2.2 to 2.2
- conv_gain: float32 [1024], P('tp'), may hold values from 0.1 to 1.9
- point_weight: bfloat16 [1024, 2048], P('tp'), may hold values from -0.1875 to 0.1875
- channel_gain: float32 [2048], replicated, may hold values from 0.1 to 1.9
- expert_ids: int32 [4096, 2], P(('grp', 'sp', 'tp')), parts along dimension 0, may hold values from 0 to 15, all different within a row; in each aligned block of 128 rows (0 to 127, 128 to 255, ...) at most 32 rows name the same one
- expert_weights: float32 [4096, 2], P(('grp', 'sp', 'tp')), parts along dimension 0, may hold values from 0.2 to 1
- gate_weight: bfloat16 [16, 2048, 768], P(('sp', 'tp')), may hold values from -0.125 to 0.125
- up_weight: bfloat16 [16, 2048, 768], P(('sp', 'tp')), may hold values from -0.125 to 0.125
- down_weight: bfloat16 [16, 768, 2048], P(('sp', 'tp')), may hold values from -0.21875 to 0.21875
Outputs:
- result: bfloat16 [4096, 2048], P(('grp', 'sp', 'tp')), parts along dimension 0
The draws below stay inside these ranges and needn't reach their ends.
There are 2 independent parts, one for each index of `grp`. The reference program is written for one: setup_inputs(seed, part) draws one part's arguments, and reference() takes and returns one part's arrays. A program takes and returns all parts, laid end to end along the dimension named above; an argument that names none is the same for every part. Nothing has to cross between parts.
Inputs may be any that keep to these rules, and one draw needn't show every extreme that they name: `expert_ids`: each row names 2 different experts. Within the rows of one device (aligned blocks of 128 rows) no expert is named by more than 32 rows, and in some device's rows some expert is named by exactly 32.
All inputs are finite; a program needn't handle non-finite values.
Results may differ from the reference program's by a relative error of at most 0.012.
Values may be sent and summed in bfloat16 or wider, within the bound.
A program may use at most 64 MiB of HBM per device.

```python
import math
import jax
import jax.numpy as jnp
import numpy as np
from jax import lax

D = 2048
CONV_WIDTH = 1024
KERNEL = 31
EXPERT_WIDTH = 768
TOP_K = 2
TOK_DEV = 128
EXPERTS = 16
TOKENS = 2048
CAP = 32


def draw_conv_taps(key, part):
    first_key, second_key = jax.random.split(jax.random.fold_in(key, 11))
    base = jax.random.truncated_normal(first_key, -3.0, 3.0, (KERNEL, CONV_WIDTH), jnp.float32)
    block_logs = jax.random.uniform(second_key, (16,), jnp.float32, -1.38, 1.38)
    channel_scale = jnp.repeat(jnp.exp(block_logs), CONV_WIDTH // 16)
    return base * KERNEL ** (-0.5) * channel_scale[None, :]


def block_scale(key, shape, cuts, least, top_value):
    level = 1.0
    for position, parts in cuts:
        steps = jax.random.uniform(jax.random.fold_in(jax.random.fold_in(key, 6), position), (parts,), jnp.float32, least / len(cuts), top_value / len(cuts))
        level = level * jnp.repeat(jnp.exp(steps), shape[position] // parts).reshape((-1,) + (1,) * (len(shape) - 1 - position))
    return level


def deal_out(own_key, own, number, rows, number_of, top, bound, skew):
    sequence = jax.random.permutation(own_key, number_of)
    heavy_load, ordinary = portions_of(number_of, rows * top, bound, skew, True), portions_of(number_of, rows * top, bound, skew, False)
    places = jnp.arange(number_of)

    def named(tallies, rotation):
        used = int((tallies > 0).sum())
        fixed = max(1, used // 4)
        passed = fixed + (places - fixed + rotation * (used - fixed)) % max(1, number_of - fixed)
        return jnp.zeros((number_of,), jnp.int32).at[sequence[jnp.where(places < fixed, places, passed)]].set(jnp.asarray(tallies, jnp.int32))

    tallies = jnp.where(number % 4 == 0, named(heavy_load, number // 4), named(ordinary, number - number // 4 - 1))
    mixed = jax.random.permutation(jax.random.fold_in(own, 3), number_of)
    source_of, receiver = mixed[0:number_of // 2 * 2:2], mixed[1:number_of // 2 * 2:2]
    margin = jnp.minimum(tallies[source_of] - 1, bound - tallies[receiver]) // 2
    margin = jnp.where((source_of == sequence[0]) | (receiver == sequence[0]) | (tallies[receiver] == 0), 0, jnp.maximum(margin, 0))
    passed = jax.random.randint(jax.random.fold_in(own, 4), (number_of // 2,), 0, 1 << 20) % (margin + 1)
    tallies = tallies.at[source_of].add(-passed).at[receiver].add(passed)
    labels = jnp.searchsorted(jnp.cumsum(tallies), jnp.arange(rows * top), side="right").astype(jnp.int32)
    grid = labels.reshape(top, rows).T
    grid = grid[jax.random.permutation(jax.random.fold_in(own, 1), rows)]
    rotation = jax.random.randint(jax.random.fold_in(own, 2), (rows, 1), 0, top)
    return jnp.take_along_axis(grid, (jnp.arange(top)[None, :] + rotation) % top, axis=1)


def portions_of(amount, total, bound, slope, full):
    weights = [(1 << 20) // math.isqrt(grade ** slope) + 1 for grade in range(1, amount + 1)]
    largest = bound if full else min(bound, max(-(-total // amount), total * weights[0] // sum(weights)))
    least = 1 if total - largest >= amount - 1 else 0
    holding, rest = [largest] + [least] * (amount - 1), total - largest - least * (amount - 1)
    while rest > 0:
        free = [i for i in range(1, amount) if holding[i] < largest] or [i for i in range(1, amount) if holding[i] < bound]
        pool, remaining = sum([weights[i] for i in free]), rest
        for i in free:
            more = min(bound - holding[i], max(1, remaining * weights[i] // pool), rest)
            holding[i] = holding[i] + more
            rest = rest - more
    return np.array(holding)


def bell_draw(rng, extent, width, limit, pieces=(), kind=jnp.bfloat16):
    result = jax.random.normal(rng, extent, jnp.float32) * width
    if len(pieces) > 0:
        result = block_scale(rng, extent, pieces, -0.22, 0.18) * result
    return jnp.clip(result, min=-limit, max=limit).astype(kind)


def setup_inputs(seed: int = 0, part: int = 0) -> dict:
    splits = jax.random.split(jax.random.key(seed), 13)
    part_splits = jax.random.split(jax.random.fold_in(splits[12], part), 13)
    latents = bell_draw(part_splits[0], (TOKENS, D), 1.0, 6.0, ((0, 16),))
    conv_value = bell_draw(part_splits[1], (TOKENS, CONV_WIDTH), 1.0, 6.0, ((0, 4), (1, 4)))
    conv_gate = bell_draw(part_splits[2], (TOKENS, CONV_WIDTH), 1.0, 6.0, ((0, 4), (1, 4)))
    conv_taps = draw_conv_taps(jax.random.fold_in(splits[12], 71), part)
    conv_gain = jnp.clip(1.0 + 0.18 * jax.random.normal(splits[4], (CONV_WIDTH,), jnp.float32), 0.1, 1.9)
    point_weight = bell_draw(splits[5], (CONV_WIDTH, D), CONV_WIDTH ** -0.5, 0.1875, ((0, 4),))
    channel_gain = jnp.clip(1.0 + 0.18 * jax.random.normal(splits[6], (D,), jnp.float32), 0.1, 1.9)
    expert_ids_keys = jax.random.split(jax.random.fold_in(part_splits[7], 1), TOKENS // TOK_DEV)
    expert_ids_turns = jax.random.permutation(jax.random.fold_in(part_splits[7], 3), TOKENS // TOK_DEV)
    expert_ids = jax.vmap(lambda own, number: deal_out(jax.random.fold_in(part_splits[7], 2), own, number, TOK_DEV, EXPERTS, TOP_K, CAP, 2))(expert_ids_keys, expert_ids_turns).reshape((TOKENS, TOP_K))
    expert_weights = jnp.clip(0.2 + 0.8 * jax.random.uniform(part_splits[8], (TOKENS, TOP_K), jnp.float32) ** block_scale(part_splits[8], (TOKENS, TOP_K), ((0, 16),), -0.2, 0.2), 0.2, 1.0)
    gate_weight = bell_draw(splits[9], (EXPERTS, D, EXPERT_WIDTH), D ** -0.5, 0.125, ((0, 16),))
    up_weight = bell_draw(splits[10], (EXPERTS, D, EXPERT_WIDTH), D ** -0.5, 0.125, ((0, 16),))
    down_weight = bell_draw(splits[11], (EXPERTS, EXPERT_WIDTH, D), EXPERT_WIDTH ** -0.5, 0.21875, ((0, 16),))
    return dict(latents=latents, conv_value=conv_value, conv_gate=conv_gate, conv_taps=conv_taps, conv_gain=conv_gain, point_weight=point_weight, channel_gain=channel_gain, expert_ids=expert_ids, expert_weights=expert_weights, gate_weight=gate_weight, up_weight=up_weight, down_weight=down_weight)


def reference(latents, conv_value, conv_gate, conv_taps, conv_gain, point_weight, channel_gain, expert_ids, expert_weights, gate_weight, up_weight, down_weight):
    gated_value = (conv_value.astype(jnp.float32) * jax.nn.sigmoid(conv_gate.astype(jnp.float32))).astype(jnp.bfloat16)
    half_span = KERNEL // 2
    padded = jnp.pad(gated_value.astype(jnp.float32), ((half_span, half_span), (0, 0)))
    tap_values = conv_taps.astype(jnp.float32)
    mixed_rows = jnp.zeros(gated_value.shape, jnp.float32)
    for offset in range(KERNEL):
        mixed_rows = mixed_rows + tap_values[offset][None, :] * padded[offset:offset + TOKENS]
    center = lax.optimization_barrier(jnp.mean(mixed_rows, axis=1, keepdims=True))
    spread = lax.optimization_barrier(jnp.mean(mixed_rows * mixed_rows, axis=1, keepdims=True)) - center * center
    activated = jax.nn.silu((mixed_rows - center) * lax.rsqrt(spread + 0.05) * conv_gain.astype(jnp.float32)).astype(jnp.bfloat16)
    branch = jnp.dot(activated, point_weight, preferred_element_type=jnp.float32)
    after_conv = (latents.astype(jnp.float32) + branch).astype(jnp.bfloat16)
    after_wide = after_conv.astype(jnp.float32)
    scale_rows = lax.rsqrt(lax.optimization_barrier(jnp.mean(after_wide * after_wide, axis=1, keepdims=True)) + 0.01)
    expert_in = (after_wide * scale_rows * channel_gain.astype(jnp.float32)).astype(jnp.bfloat16)
    blocks = TOKENS // TOK_DEV
    expert_slots = blocks * CAP
    flat_ids = expert_ids.astype(jnp.int32).reshape(blocks, TOK_DEV * TOP_K)
    onehot = (flat_ids[:, :, None] == jnp.arange(EXPERTS, dtype=jnp.int32)[None, None, :]).astype(jnp.int32)
    earlier = lax.optimization_barrier(jnp.sum((jnp.cumsum(onehot, axis=1) - onehot) * onehot, axis=2))
    block_index = jnp.arange(blocks, dtype=jnp.int32)[:, None]
    target = (flat_ids * expert_slots + block_index * CAP + earlier).reshape(-1).astype(jnp.int32)
    token_index = jnp.repeat(jnp.arange(TOKENS, dtype=jnp.int32), TOP_K)
    slot_table = jnp.full((EXPERTS * expert_slots,), TOKENS, jnp.int32).at[target].set(token_index)
    slot_table = slot_table.reshape(EXPERTS, expert_slots)
    padded_in = jnp.concatenate([expert_in, jnp.zeros((1, expert_in.shape[1]), jnp.bfloat16)], axis=0)

    def one_expert(operands):
        row_index, gate_rows, up_rows, down_rows = operands
        chosen = padded_in[row_index]
        gate_part = jnp.dot(chosen, gate_rows, preferred_element_type=jnp.float32)
        up_part = jnp.dot(chosen, up_rows, preferred_element_type=jnp.float32)
        hidden = (jax.nn.silu(gate_part) * up_part).astype(jnp.bfloat16)
        return jnp.dot(hidden, down_rows, preferred_element_type=jnp.float32).astype(jnp.bfloat16)
    outputs = lax.map(one_expert, (slot_table, gate_weight, up_weight, down_weight))
    picked = outputs.reshape(EXPERTS * expert_slots, -1)[target].astype(jnp.float32).reshape(TOKENS, TOP_K, -1)
    routed = lax.optimization_barrier(jnp.sum(expert_weights.astype(jnp.float32)[:, :, None] * picked, axis=1))
    return (after_wide + routed).astype(jnp.bfloat16)
```

```python
import functools

import jax
import jax.numpy as jnp
from jax import lax
from jax.experimental import pallas as pl
from jax.experimental.pallas import tpu as pltpu
from jax.sharding import PartitionSpec as P


MESH = pl.DeviceIdType.MESH
PARTS = 4
BANDS = 4


def layer_kernel(
    n, tp, taps_count, cap,
    value_hbm, gate_hbm, taps_hbm, cgain_hbm, weight_hbm, latent_hbm, gain_hbm, ids_hbm, share_hbm,
    wg_hbm, wu_hbm, wd_hbm, out_ref,
    value_ref, gate_ref, taps_ref, cgain_ref, gain_ref, ids_ref, share_ref,
    gated, wide, mixed, stats, act_out, act_in, psend,
    toks, tabs, comp, arr, back, inc, acc, wg, wu, wd, ga, ua, hid,
    load_sem, point_sem, w_sem, halo_send, halo_recv, stat_send, stat_recv, mate_send, mate_recv,
    act_send, act_recv, part_send, part_recv,
    tok_send, tok_recv, tab_send, tab_recv,
    piece_send, piece_recv, back_send, back_recv, sum_send, sum_recv,
):
    z = lax.axis_index("sp")
    t = lax.axis_index("tp")
    block, chans = value_ref.shape
    rows, width = out_ref.shape
    slots = tp * cap
    hidden_width = wg.shape[1]
    top_count = ids_ref.shape[0]
    cols = width // PARTS
    band_rows = rows // BANDS
    half = taps_count // 2
    edge = (gated.shape[0] - block) // 2
    view = rows + 2 * edge
    q_count = tp // 2
    core = lax.rem(t, 2)
    quad = t // 2
    mate = t + 1 - 2 * core
    chunks = chans // rows
    base = 2 * chunks

    def col(c):
        return pl.ds(c * cols, cols)

    loads = [
        pltpu.make_async_copy(a, b, load_sem.at[i])
        for i, (a, b) in enumerate(
            (
                (value_hbm, value_ref),
                (gate_hbm, gate_ref),
                (taps_hbm, taps_ref),
                (cgain_hbm, cgain_ref),
                (ids_hbm, ids_ref),
                (share_hbm, share_ref),
                (gain_hbm, gain_ref),
                (latent_hbm, out_ref),
            )
        )
    ]
    for load in loads:
        load.start()

    point_loads = [
        pltpu.make_async_copy(
            weight_hbm.at[pl.ds(b * rows, rows), col(c)],
            inc.at[core * chunks + b, c],
            point_sem.at[b, c],
        )
        for b in range(chunks)
        for c in range(PARTS)
    ]
    for load in point_loads:
        load.start()

    barrier = pltpu.get_barrier_semaphore()
    for p in range(1, tp):
        pl.semaphore_signal(
            barrier, inc=1, device_id={"tp": lax.rem(t + p, tp)}, device_id_type=MESH
        )

    @pl.when(z > 0)
    def _():
        pl.semaphore_signal(barrier, inc=1, device_id={"sp": z - 1}, device_id_type=MESH)

    @pl.when(z < n - 1)
    def _():
        pl.semaphore_signal(barrier, inc=1, device_id={"sp": z + 1}, device_id_type=MESH)

    @pl.when(z == 0)
    def _():
        gated[pl.ds(0, edge)] = jnp.zeros((edge, chans), jnp.bfloat16)

    @pl.when(z == n - 1)
    def _():
        gated[pl.ds(edge + block, edge)] = jnp.zeros((edge, chans), jnp.bfloat16)

    loads[0].wait()
    loads[1].wait()
    step = 64
    for r in range(0, block, step):
        value = value_ref[pl.ds(r, step)].astype(jnp.float32)
        gate = gate_ref[pl.ds(r, step)].astype(jnp.float32)
        gated[pl.ds(edge + r, step)] = (value * jax.nn.sigmoid(gate)).astype(jnp.bfloat16)

    peers = tp - 1 + (z > 0).astype(jnp.int32) + (z < n - 1).astype(jnp.int32)
    pl.semaphore_wait(barrier, peers)

    def halo_copy(up):
        start = block if up else edge
        place = 0 if up else edge + block
        return pltpu.make_async_remote_copy(
            src_ref=gated.at[pl.ds(start, edge)], dst_ref=gated.at[pl.ds(place, edge)],
            send_sem=halo_send.at[up], recv_sem=halo_recv.at[up],
            device_id={"sp": z + 1 if up else z - 1}, device_id_type=MESH,
        )

    @pl.when(z < n - 1)
    def _():
        halo_copy(1).start()

    @pl.when(z > 0)
    def _():
        halo_copy(0).start()

    for load in point_loads:
        load.wait()
    own_rows = pl.ds(core * chunks, chunks)
    mate_copy = pltpu.make_async_remote_copy(
        src_ref=inc.at[own_rows], dst_ref=inc.at[own_rows],
        send_sem=mate_send.at[0], recv_sem=mate_recv.at[0],
        device_id={"tp": mate}, device_id_type=MESH,
    )
    mate_copy.start()

    expert_loads = [
        pltpu.make_async_copy(a, b, w_sem.at[i])
        for i, (a, b) in enumerate(((wg_hbm.at[0], wg), (wu_hbm.at[0], wu), (wd_hbm.at[0], wd)))
    ]
    for load in expert_loads:
        load.start()
    for load in loads[2:]:
        load.wait()

    def convolve(s):
        wide[...] = gated[pl.ds(pl.multiple_of(s * rows, 16), view)].astype(jnp.float32)
        tile = 64
        sums, squares = [], []
        for r in range(0, rows, tile):
            value = jnp.zeros((tile, chans), jnp.float32)
            for i in range(taps_count):
                value = value + taps_ref[pl.ds(i, 1)] * wide[pl.ds(edge - half + i + r, tile)]
            mixed[s, pl.ds(r, tile)] = value
            sums.append(jnp.sum(value, axis=1, keepdims=True))
            squares.append(jnp.sum(value * value, axis=1, keepdims=True))
        for k, parts in enumerate((sums, squares)):
            line = jnp.broadcast_to(jnp.concatenate(parts, axis=0), (rows, rows)).T
            stats[t, s, pl.ds(k, 1)] = line[0:1]

    def inner(i, carry):
        convolve(i + 1)
        return carry

    lax.fori_loop(0, tp - 2, inner, 0)

    @pl.when(z > 0)
    def _():
        halo_copy(1).wait_recv()

    @pl.when(z < n - 1)
    def _():
        halo_copy(0).wait_recv()

    def outer(i, carry):
        convolve(i * (tp - 1))
        return carry

    lax.fori_loop(0, 2, outer, 0)

    def stat_copy(p):
        return pltpu.make_async_remote_copy(
            src_ref=stats.at[t], dst_ref=stats.at[t],
            send_sem=stat_send.at[p], recv_sem=stat_recv.at[t],
            device_id={"tp": lax.rem(t + p, tp)}, device_id_type=MESH,
        )

    for p in range(1, tp):
        stat_copy(p).start()

    ids = ids_ref[...].astype(jnp.float32)
    across = [jnp.broadcast_to(ids[k : k + 1], (rows, rows)) for k in range(top_count)]
    down = [value.T for value in across]
    down_place = lax.broadcasted_iota(jnp.int32, (rows, rows), 0)
    across_place = lax.broadcasted_iota(jnp.int32, (rows, rows), 1)
    tabs[z] = jnp.zeros(tabs.shape[1:], jnp.float32)
    for k in range(top_count):
        count = jnp.zeros((1, rows), jnp.float32)
        for m in range(k + 1):
            same = down[m] == across[k]
            if m == k:
                same = same & (down_place < across_place)
            count = count + jnp.sum(jnp.where(same, 1.0, 0.0), axis=0, keepdims=True)
        tabs[z, pl.ds(k, 1)] = ids[k : k + 1] * cap + count
        tabs[z, pl.ds(top_count + k, 1)] = share_ref[pl.ds(k, 1)]

    for p in range(1, tp):
        other = lax.rem(t + p, tp)
        pltpu.make_async_copy(stats.at[other], stats.at[other], stat_recv.at[other]).wait()

    def activate(s):
        both = stats[0, s]
        for p in range(1, tp):
            both = both + stats[p, s]
        both = both / (chans * tp)
        center = both[0:1]
        scale = lax.rsqrt(both[1:2] - center * center + 0.05)
        center = jnp.broadcast_to(center, (rows, rows)).T[:, 0:1]
        scale = jnp.broadcast_to(scale, (rows, rows)).T[:, 0:1]
        value = (mixed[s] - center) * scale * cgain_ref[...]
        return jax.nn.silu(value).astype(jnp.bfloat16)

    def act_copy(i):
        spot = lax.rem(quad + i, q_count)
        return pltpu.make_async_remote_copy(
            src_ref=act_out.at[spot], dst_ref=act_in.at[spot, core],
            send_sem=act_send.at[i], recv_sem=act_recv.at[spot],
            device_id={"tp": mate}, device_id_type=MESH,
        )

    order = list(range(1, q_count)) + [0]
    for i in order:
        spot = lax.rem(quad + i, q_count)
        act_out[spot] = activate(2 * spot + 1 - core)
        act_copy(i).start()
    for i in order:
        spot = lax.rem(quad + i, q_count)
        act_in[spot, core] = activate(2 * spot + core)

    mate_copy.wait()

    def product(i, c):
        spot = lax.rem(quad + i, q_count)
        left = jnp.concatenate([act_in[spot, 0], act_in[spot, 1]], axis=1)
        right = inc[pl.ds(0, base), c].reshape(base * rows, cols)
        return jnp.dot(left, right, preferred_element_type=jnp.float32)

    def part_copy(i, k):
        piece = pl.ds(k * band_rows, band_rows)
        return pltpu.make_async_remote_copy(
            src_ref=psend.at[i - 1, :, piece], dst_ref=inc.at[base + i - 1, :, piece],
            send_sem=part_send.at[i - 1, k], recv_sem=part_recv.at[i - 1, k],
            device_id={"tp": 2 * lax.rem(quad + i, q_count) + core}, device_id_type=MESH,
        )

    for i in order:
        spot = lax.rem(quad + i, q_count)
        pltpu.make_async_copy(act_out.at[spot], act_out.at[spot], act_recv.at[spot]).wait()
        for c in range(PARTS):
            if i:
                psend[i - 1, c] = product(i, c).astype(jnp.bfloat16)
            else:
                acc[c] = product(i, c)
        if i:
            for k in range(BANDS):
                part_copy(i, k).start()

    def token_copy(zs, k, side):
        piece = pl.ds(k * band_rows, band_rows)
        return pltpu.make_async_remote_copy(
            src_ref=toks.at[zs, :, piece], dst_ref=toks.at[zs, :, piece],
            send_sem=tok_send.at[side, zs, k], recv_sem=tok_recv.at[zs, k],
            device_id={"sp": z + 1 if side else z - 1}, device_id_type=MESH,
        )

    def table_copy(zs, side):
        return pltpu.make_async_remote_copy(
            src_ref=tabs.at[zs], dst_ref=tabs.at[zs],
            send_sem=tab_send.at[side, zs], recv_sem=tab_recv.at[zs],
            device_id={"sp": z + 1 if side else z - 1}, device_id_type=MESH,
        )

    def each_side(zs, act):
        @pl.when((zs <= z) & (z < n - 1))
        def _():
            act(1)

        @pl.when((zs >= z) & (z > 0))
        def _():
            act(0)

    each_side(z, lambda side: table_copy(z, side).start())

    for k in range(BANDS):
        piece = pl.ds(k * band_rows, band_rows)
        for i in range(1, q_count):
            spot = inc.at[base + i - 1, :, piece]
            pltpu.make_async_copy(spot, spot, part_recv.at[i - 1, k]).wait()
        square = jnp.zeros((band_rows, 1), jnp.float32)
        for c in range(PARTS):
            total = acc[c, piece] + out_ref[piece, col(c)].astype(jnp.float32)
            for i in range(1, q_count):
                total = total + inc[base + i - 1, c, piece].astype(jnp.float32)
            after = total.astype(jnp.bfloat16)
            out_ref[piece, col(c)] = after
            after = after.astype(jnp.float32)
            square = square + jnp.sum(after * after, axis=1, keepdims=True)
        norm = lax.rsqrt(square / width + 0.01)
        for c in range(PARTS):
            after = out_ref[piece, col(c)].astype(jnp.float32)
            toks[z, c, piece] = (after * norm * gain_ref[:, col(c)]).astype(jnp.bfloat16)
        each_side(z, lambda side: token_copy(z, k, side).start())


    def source(j):
        low = jnp.minimum(z, n - 1 - z)
        near = jnp.where(j % 2 == 1, z - (j + 1) // 2, z + j // 2)
        far = jnp.where(z > n - 1 - z, z - (j - low), z + (j - low))
        return jnp.where(j <= 2 * low, near, far)

    def span(index):
        return pl.ds(pl.multiple_of(index * cap, 16), cap)

    def exchange(j, c, to_ref, zs, ss, rs):
        page = lax.rem(j, 2)
        for p in range(1, tp):
            other = lax.rem(t + p, tp)
            pltpu.make_async_remote_copy(
                src_ref=comp.at[page, c, span(other)],
                dst_ref=to_ref.at[zs, c, span(t)],
                send_sem=ss.at[zs, c],
                recv_sem=rs.at[zs, c],
                device_id={"tp": other},
                device_id_type=MESH,
            ).start()
        to_ref[zs, c, span(t)] = comp[page, c, span(t)]

    def wait_pieces(ref, zs, c, ss, rs):
        part = ref.at[zs, c, pl.ds(0, (tp - 1) * cap)]
        pltpu.make_async_copy(part, part, rs.at[zs, c]).wait()
        pltpu.make_async_copy(part, part, ss.at[zs, c]).wait()

    def sum_copy(zs, c, side):
        target = z + 1 if side else z - 1
        slot = jnp.where(target == zs, n, zs) if side else zs
        return pltpu.make_async_remote_copy(
            src_ref=toks.at[zs, c],
            dst_ref=inc.at[slot, c],
            send_sem=sum_send.at[zs, c],
            recv_sem=sum_recv.at[slot, c],
            device_id={"sp": target},
            device_id_type=MESH,
        )

    def names(zs):
        table = tabs[zs]
        start = (z * slots).astype(jnp.float32)
        place = lax.broadcasted_iota(jnp.int32, (slots, rows), 0).astype(jnp.float32) + start
        return place == table[0:1, :], place == table[1:2, :], table

    def passes_on(zs):
        return ((zs < z) & (z < n - 1)) | ((zs > z) & (z > 0))

    def arrive(zs, k):
        spot = toks.at[zs, :, pl.ds(k * band_rows, band_rows)]
        pltpu.make_async_copy(spot, spot, tok_recv.at[zs, k]).wait()

    def hand_on(j):
        zs = source(jnp.minimum(j, n - 1))

        @pl.when((j < n) & passes_on(zs))
        def _():
            pltpu.make_async_copy(tabs.at[zs], tabs.at[zs], tab_recv.at[zs]).wait()
            each_side(zs, lambda side: table_copy(zs, side).start())
            for k in range(BANDS):
                arrive(zs, k)
                each_side(zs, lambda side: token_copy(zs, k, side).start())

    def take(j):
        zs = source(j)

        @pl.when((zs != z) & jnp.logical_not(passes_on(zs)))
        def _():
            pltpu.make_async_copy(tabs.at[zs], tabs.at[zs], tab_recv.at[zs]).wait()
            for k in range(BANDS):
                arrive(zs, k)

        first, second, _ = names(zs)
        pick = jnp.where(first | second, 1.0, 0.0).astype(jnp.bfloat16)
        page = lax.rem(j, 2)
        for c in range(PARTS):
            comp[page, c] = jnp.dot(
                pick, toks[zs, c], preferred_element_type=jnp.float32
            ).astype(jnp.bfloat16)
            exchange(j, c, arr, zs, piece_send, piece_recv)

    def run(j):
        zs = source(j)

        @pl.when(j == 0)
        def _():
            for load in expert_loads:
                load.wait()

        step = 256
        for c in range(PARTS):
            wait_pieces(arr, zs, c, piece_send, piece_recv)
            for f in range(0, hidden_width, step):
                for to, weights in ((ga, wg), (ua, wu)):
                    value = jnp.dot(
                        arr[zs, c], weights[col(c), f : f + step],
                        preferred_element_type=jnp.float32,
                    )
                    if c:
                        value = value + to[:, f : f + step]
                    if c < PARTS - 1 or to is ga:
                        to[:, f : f + step] = value
                if c == PARTS - 1:
                    gate = ga[:, f : f + step]
                    hid[:, f : f + step] = (jax.nn.silu(gate) * value).astype(jnp.bfloat16)
        page = lax.rem(j, 2)
        for c in range(PARTS):
            comp[page, c] = jnp.dot(
                hid[...], wd[:, col(c)], preferred_element_type=jnp.float32
            ).astype(jnp.bfloat16)
            exchange(j, c, back, zs, back_send, back_recv)

    def merge(j):
        zs = source(j)
        first, second, table = names(zs)
        share = jnp.where(first, table[2:3, :], 0.0) + jnp.where(second, table[3:4, :], 0.0)
        share = share.T
        high = share.astype(jnp.bfloat16)
        rest = (share - high.astype(jnp.float32)).astype(jnp.bfloat16)

        def sent(side):
            table_copy(zs, side).wait_send()
            for k in range(BANDS):
                token_copy(zs, k, side).wait_send()

        each_side(zs, sent)
        for c in range(PARTS):
            wait_pieces(back, zs, c, back_send, back_recv)
            value = jnp.dot(high, back[zs, c], preferred_element_type=jnp.float32) + jnp.dot(
                rest, back[zs, c], preferred_element_type=jnp.float32
            )

            @pl.when(zs == z)
            def _():
                acc[c] = value

            @pl.when(zs != z)
            def _():
                toks[zs, c] = value.astype(jnp.bfloat16)

            @pl.when((zs < z) & (z == n - 1))
            def _():
                sum_copy(zs, c, 0).start()

            @pl.when((zs > z) & (z == 0))
            def _():
                sum_copy(zs, c, 1).start()

    upper = z > n - 1 - z

    def relay(turn):
        def pass_sum(zs, side, c):
            spot = inc.at[zs, c]
            pltpu.make_async_copy(spot, spot, sum_recv.at[zs, c]).wait()
            toks[zs, c] = (
                toks[zs, c].astype(jnp.float32) + inc[zs, c].astype(jnp.float32)
            ).astype(jnp.bfloat16)
            sum_copy(zs, c, side).start()

        def go_up(c):
            @pl.when((z > 0) & (z < turn))
            def _():
                pass_sum(turn, 1, c)

        def go_down(c):
            @pl.when((z < n - 1) & (z > n - 1 - turn))
            def _():
                pass_sum(n - 1 - turn, 0, c)

        for c in range(PARTS):
            @pl.when(upper)
            def _():
                go_down(c)

            go_up(c)

            @pl.when(jnp.logical_not(upper))
            def _():
                go_down(c)

    def body(j, carry):
        @pl.when(j == 1)
        def _():
            hand_on(j)

        @pl.when(j > 0)
        def _():
            hand_on(j + 1)

        @pl.when(j < n)
        def _():
            take(j)

        @pl.when((j > 0) & (j <= n))
        def _():
            merge(j - 1)

        @pl.when(j < n)
        def _():
            run(j)

        @pl.when(j > 2)
        def _():
            relay(j - 2)

        return carry

    lax.fori_loop(0, n + 2, body, 0)

    for c in range(PARTS):
        @pl.when(z < n - 1)
        def _():
            spot = inc.at[z, c]
            pltpu.make_async_copy(spot, spot, sum_recv.at[z, c]).wait()
            acc[c] = acc[c] + inc[z, c].astype(jnp.float32)

        @pl.when(z > 0)
        def _():
            spot = inc.at[n, c]
            pltpu.make_async_copy(spot, spot, sum_recv.at[n, c]).wait()
            acc[c] = acc[c] + inc[n, c].astype(jnp.float32)

        out_ref[:, col(c)] = (out_ref[:, col(c)].astype(jnp.float32) + acc[c]).astype(jnp.bfloat16)

    def drain(zs, carry):
        @pl.when(zs != z)
        def _():
            for c in range(PARTS):
                spot = toks.at[zs, c]
                pltpu.make_async_copy(spot, spot, sum_send.at[zs, c]).wait()

        return carry

    lax.fori_loop(0, n, drain, 0)
    for p in range(1, tp):
        stat_copy(p).wait_send()
    for i in order:
        act_copy(i).wait_send()
        if i:
            for k in range(BANDS):
                part_copy(i, k).wait_send()

    @pl.when(z < n - 1)
    def _():
        halo_copy(1).wait_send()

    @pl.when(z > 0)
    def _():
        halo_copy(0).wait_send()


def shards(
    latents,
    conv_value,
    conv_gate,
    conv_taps,
    conv_gain,
    point_weight,
    channel_gain,
    expert_ids,
    expert_weights,
    gate_weight,
    up_weight,
    down_weight,
):
    n, tp = lax.axis_size("sp"), lax.axis_size("tp")
    rows, top_count = expert_ids.shape
    experts = gate_weight.shape[0] * n * tp
    cap = -(-(2 * top_count * rows // experts) // 16) * 16
    block, chans = conv_value.shape
    width = latents.shape[1]
    taps_count = conv_taps.shape[0]
    hidden_width = gate_weight.shape[2]
    slots = tp * cap
    cols = width // PARTS
    edge = -(-(taps_count // 2) // 16) * 16
    q_count = tp // 2
    spots = max(n + 1, 2 * chans // rows + q_count - 1)
    dma = pltpu.SemaphoreType.DMA
    bf16, f32 = jnp.bfloat16, jnp.float32
    anywhere = pl.BlockSpec(memory_space=pl.ANY)
    vmem = pltpu.VMEM
    return pl.pallas_call(
        functools.partial(layer_kernel, n, tp, taps_count, cap),
        out_shape=jax.ShapeDtypeStruct((rows, width), bf16),
        in_specs=[anywhere] * 12,
        out_specs=pl.BlockSpec(memory_space=pltpu.VMEM),
        scratch_shapes=[
            vmem((block, chans), bf16),
            vmem((block, chans), bf16),
            vmem((taps_count, chans), f32),
            vmem((1, chans), f32),
            vmem((1, width), f32),
            vmem((top_count, rows), jnp.int32),
            vmem((top_count, rows), f32),
            vmem((block + 2 * edge, chans), bf16),
            vmem((rows + 2 * edge, chans), f32),
            vmem((tp, rows, chans), f32),
            vmem((tp, tp, 8, rows), f32),
            vmem((q_count, rows, chans), bf16),
            vmem((q_count, 2, rows, chans), bf16),
            vmem((q_count - 1, PARTS, rows, cols), bf16),
            vmem((n, PARTS, rows, cols), bf16),
            vmem((n, 8, rows), f32),
            vmem((2, PARTS, slots, cols), bf16),
            vmem((n, PARTS, slots, cols), bf16),
            vmem((n, PARTS, slots, cols), bf16),
            vmem((spots, PARTS, rows, cols), bf16),
            vmem((PARTS, rows, cols), f32),
            vmem((width, hidden_width), bf16),
            vmem((width, hidden_width), bf16),
            vmem((hidden_width, width), bf16),
            vmem((slots, hidden_width), f32),
            vmem((slots, hidden_width), f32),
            vmem((slots, hidden_width), bf16),
            dma((8,)),
            dma((chans // rows, PARTS)),
            dma((3,)),
            dma((2,)),
            dma((2,)),
            dma((tp,)),
            dma((tp,)),
            dma((1,)),
            dma((1,)),
            dma((q_count,)),
            dma((q_count,)),
            dma((q_count - 1, BANDS)),
            dma((q_count - 1, BANDS)),
            dma((2, n, BANDS)),
            dma((n, BANDS)),
            dma((2, n)),
            dma((n,)),
            dma((n, PARTS)),
            dma((n, PARTS)),
            dma((n, PARTS)),
            dma((n, PARTS)),
            dma((n, PARTS)),
            dma((n + 1, PARTS)),
        ],
        compiler_params=pltpu.CompilerParams(
            collective_id=0, has_side_effects=True, vmem_limit_bytes=67043328
        ),
        name="layer",
    )(
        conv_value, conv_gate, conv_taps, conv_gain[None, :], point_weight, latents,
        channel_gain[None, :], expert_ids.T, expert_weights.T,
        gate_weight, up_weight, down_weight,
    )


def solution(mesh):
    return jax.shard_map(
        shards,
        mesh=mesh,
        in_specs=(
            P(("grp", "sp", "tp"), None),
            P(("grp", "sp"), "tp"),
            P(("grp", "sp"), "tp"),
            P(None, "tp"),
            P("tp"),
            P("tp", None),
            P(),
            P(("grp", "sp", "tp"), None),
            P(("grp", "sp", "tp"), None),
            P(("sp", "tp"), None, None),
            P(("sp", "tp"), None, None),
            P(("sp", "tp"), None, None),
        ),
        out_specs=P(("grp", "sp", "tp"), None),
        check_vma=False,
    )
```

```python
import functools

import jax
import jax.numpy as jnp
from jax import lax
from jax.experimental import pallas as pl
from jax.experimental.pallas import tpu as pltpu
from jax.sharding import PartitionSpec as P


MESH = pl.DeviceIdType.MESH
PARTS = 4
BANDS = (0, 1, 2, 3, 4, 5, 6, 7, 8)
SPLIT = 2
LAG = 3
PAGES = 3


def layer_kernel(
    n, tp, taps_count, cap,
    value_hbm, gate_hbm, taps_hbm, cgain_hbm, weight_hbm, latent_hbm, gain_hbm, ids_hbm, share_hbm,
    wg_hbm, wu_hbm, wd_hbm, out_hbm,
    value_ref, gate_ref, taps_ref, cgain_ref, gain_ref, ids_ref, share_ref,
    kept, gated, wide, mixed, stats, act_out, act_in, psend,
    toks, tabs, comp, arr, back, inc, acc, wg, wu, wd, ga, ua, hid,
    load_sem, point_sem, w_sem, out_sem, halo_send, halo_recv, stat_send, stat_recv, mate_send, mate_recv,
    act_send, act_recv, part_send, part_recv,
    tok_send, tok_recv, tab_send, tab_recv,
    piece_send, piece_recv, back_send, back_recv, sum_send, sum_recv,
):
    z = lax.axis_index("sp")
    t = lax.axis_index("tp")
    block, chans = value_ref.shape
    rows, width = kept.shape
    slots = tp * cap
    hidden_width = wg.shape[1]
    top_count = ids_ref.shape[0]
    cols = width // PARTS
    half = taps_count // 2
    edge = (gated.shape[0] - block) // 2
    view = rows + 2 * edge
    q_count = tp // 2
    core = lax.rem(t, 2)
    quad = t // 2
    mate = t + 1 - 2 * core
    chunks = chans // rows
    base = 2 * chunks

    def band(k):
        return pl.ds(BANDS[k] * rows // BANDS[-1], (BANDS[k + 1] - BANDS[k]) * rows // BANDS[-1])

    def col(c):
        return pl.ds(c * cols, cols)

    loads = [
        pltpu.make_async_copy(a, b, load_sem.at[i])
        for i, (a, b) in enumerate(
            (
                (value_hbm, value_ref),
                (gate_hbm, gate_ref),
                (taps_hbm, taps_ref),
                (cgain_hbm, cgain_ref),
                (ids_hbm, ids_ref),
                (share_hbm, share_ref),
                (gain_hbm, gain_ref),
                (latent_hbm, kept),
            )
        )
    ]
    for load in loads:
        load.start()

    point_loads = [
        pltpu.make_async_copy(
            weight_hbm.at[pl.ds(b * rows, rows), col(c)],
            inc.at[core * chunks + b, c],
            point_sem.at[0],
        )
        for b in range(chunks)
        for c in range(PARTS)
    ]
    for load in point_loads:
        load.start()

    barrier = pltpu.get_barrier_semaphore()
    for p in range(1, tp):
        pl.semaphore_signal(
            barrier, inc=1, device_id={"tp": lax.rem(t + p, tp)}, device_id_type=MESH
        )

    @pl.when(z > 0)
    def _():
        pl.semaphore_signal(barrier, inc=1, device_id={"sp": z - 1}, device_id_type=MESH)

    @pl.when(z < n - 1)
    def _():
        pl.semaphore_signal(barrier, inc=1, device_id={"sp": z + 1}, device_id_type=MESH)

    @pl.when(z == 0)
    def _():
        gated[pl.ds(0, edge)] = jnp.zeros((edge, chans), jnp.bfloat16)

    @pl.when(z == n - 1)
    def _():
        gated[pl.ds(edge + block, edge)] = jnp.zeros((edge, chans), jnp.bfloat16)

    loads[0].wait()
    loads[1].wait()
    step = 64
    for r in range(0, block, step):
        value = value_ref[pl.ds(r, step)].astype(jnp.float32)
        gate = gate_ref[pl.ds(r, step)].astype(jnp.float32)
        gated[pl.ds(edge + r, step)] = (value * jax.nn.sigmoid(gate)).astype(jnp.bfloat16)

    peers = tp - 1 + (z > 0).astype(jnp.int32) + (z < n - 1).astype(jnp.int32)
    pl.semaphore_wait(barrier, peers)

    def halo_copy(up):
        start = block if up else edge
        place = 0 if up else edge + block
        return pltpu.make_async_remote_copy(
            src_ref=gated.at[pl.ds(start, edge)], dst_ref=gated.at[pl.ds(place, edge)],
            send_sem=halo_send.at[up], recv_sem=halo_recv.at[up],
            device_id={"sp": z + 1 if up else z - 1}, device_id_type=MESH,
        )

    @pl.when(z < n - 1)
    def _():
        halo_copy(1).start()

    @pl.when(z > 0)
    def _():
        halo_copy(0).start()

    own_rows = pl.ds(core * chunks, chunks)
    pltpu.make_async_copy(inc.at[own_rows], inc.at[own_rows], point_sem.at[0]).wait()
    mate_copy = pltpu.make_async_remote_copy(
        src_ref=inc.at[own_rows], dst_ref=inc.at[own_rows],
        send_sem=mate_send.at[0], recv_sem=mate_recv.at[0],
        device_id={"tp": mate}, device_id_type=MESH,
    )
    mate_copy.start()

    expert_loads = [
        pltpu.make_async_copy(a, b, w_sem.at[i])
        for i, (a, b) in enumerate(((wg_hbm.at[0], wg), (wu_hbm.at[0], wu), (wd_hbm.at[0], wd)))
    ]
    for load in expert_loads:
        load.start()
    for load in loads[2:]:
        load.wait()

    def convolve(s):
        wide[...] = gated[pl.ds(pl.multiple_of(s * rows, 16), view)].astype(jnp.float32)
        tile = 64
        sums, squares = [], []
        for r in range(0, rows, tile):
            value = jnp.zeros((tile, chans), jnp.float32)
            for i in range(taps_count):
                value = value + taps_ref[pl.ds(i, 1)] * wide[pl.ds(edge - half + i + r, tile)]
            mixed[s, pl.ds(r, tile)] = value
            sums.append(jnp.sum(value, axis=1, keepdims=True))
            squares.append(jnp.sum(value * value, axis=1, keepdims=True))
        for k, parts in enumerate((sums, squares)):
            line = jnp.broadcast_to(jnp.concatenate(parts, axis=0), (rows, rows)).T
            stats[t, s, pl.ds(k, 1)] = line[0:1]

    def inner(i, carry):
        convolve(i + 1)
        return carry

    lax.fori_loop(0, tp - 2, inner, 0)

    @pl.when(z > 0)
    def _():
        halo_copy(1).wait_recv()

    @pl.when(z < n - 1)
    def _():
        halo_copy(0).wait_recv()

    def outer(i, carry):
        convolve(i * (tp - 1))
        return carry

    lax.fori_loop(0, 2, outer, 0)

    def stat_copy(p):
        return pltpu.make_async_remote_copy(
            src_ref=stats.at[t], dst_ref=stats.at[t],
            send_sem=stat_send.at[0], recv_sem=stat_recv.at[0],
            device_id={"tp": lax.rem(t + p, tp)}, device_id_type=MESH,
        )

    for p in range(1, tp):
        stat_copy(p).start()

    ids = ids_ref[...].astype(jnp.float32)
    across = [jnp.broadcast_to(ids[k : k + 1], (rows, rows)) for k in range(top_count)]
    down = [value.T for value in across]
    down_place = lax.broadcasted_iota(jnp.int32, (rows, rows), 0)
    across_place = lax.broadcasted_iota(jnp.int32, (rows, rows), 1)
    tabs[z] = jnp.zeros(tabs.shape[1:], jnp.float32)
    for k in range(top_count):
        count = jnp.zeros((1, rows), jnp.float32)
        for m in range(k + 1):
            same = down[m] == across[k]
            if m == k:
                same = same & (down_place < across_place)
            count = count + jnp.sum(jnp.where(same, 1.0, 0.0), axis=0, keepdims=True)
        tabs[z, pl.ds(k, 1)] = ids[k : k + 1] * cap + count
        tabs[z, pl.ds(top_count + k, 1)] = share_ref[pl.ds(k, 1)]

    others = stats.at[pl.ds(0, tp - 1)]
    pltpu.make_async_copy(others, others, stat_recv.at[0]).wait()

    def activate(s):
        both = stats[0, s]
        for p in range(1, tp):
            both = both + stats[p, s]
        both = both / (chans * tp)
        center = both[0:1]
        scale = lax.rsqrt(both[1:2] - center * center + 0.05)
        center = jnp.broadcast_to(center, (rows, rows)).T[:, 0:1]
        scale = jnp.broadcast_to(scale, (rows, rows)).T[:, 0:1]
        value = (mixed[s] - center) * scale * cgain_ref[...]
        return jax.nn.silu(value).astype(jnp.bfloat16)

    def act_copy(i):
        spot = lax.rem(quad + i, q_count)
        return pltpu.make_async_remote_copy(
            src_ref=act_out.at[spot], dst_ref=act_in.at[spot, core],
            send_sem=act_send.at[i], recv_sem=act_recv.at[spot],
            device_id={"tp": mate}, device_id_type=MESH,
        )

    order = list(range(1, q_count)) + [0]
    for i in order:
        spot = lax.rem(quad + i, q_count)
        act_out[spot] = activate(2 * spot + 1 - core)
        act_copy(i).start()
    for i in order:
        spot = lax.rem(quad + i, q_count)
        act_in[spot, core] = activate(2 * spot + core)

    mate_copy.wait()

    def product(i, c):
        spot = lax.rem(quad + i, q_count)
        left = jnp.concatenate([act_in[spot, 0], act_in[spot, 1]], axis=1)
        right = inc[pl.ds(0, base), c].reshape(base * rows, cols)
        return jnp.dot(left, right, preferred_element_type=jnp.float32)

    def part_copy(i, k):
        piece = band(k)
        return pltpu.make_async_remote_copy(
            src_ref=psend.at[i - 1, :, piece], dst_ref=inc.at[base + i - 1, :, piece],
            send_sem=part_send.at[i - 1], recv_sem=part_recv.at[i - 1, k],
            device_id={"tp": 2 * lax.rem(quad + i, q_count) + core}, device_id_type=MESH,
        )

    for i in order:
        spot = lax.rem(quad + i, q_count)
        pltpu.make_async_copy(act_out.at[spot], act_out.at[spot], act_recv.at[spot]).wait()
        for c in range(PARTS):
            if i:
                psend[i - 1, c] = product(i, c).astype(jnp.bfloat16)
            else:
                acc[c] = product(i, c)
        if i:
            for k in range(len(BANDS) - 1):
                part_copy(i, k).start()

    def token_copy(zs, k, side):
        piece = band(k)
        return pltpu.make_async_remote_copy(
            src_ref=toks.at[zs, :, piece], dst_ref=toks.at[zs, :, piece],
            send_sem=tok_send.at[side, zs], recv_sem=tok_recv.at[zs, k],
            device_id={"sp": z + 1 if side else z - 1}, device_id_type=MESH,
        )

    def table_copy(zs, side):
        return pltpu.make_async_remote_copy(
            src_ref=tabs.at[zs], dst_ref=tabs.at[zs],
            send_sem=tab_send.at[side, zs], recv_sem=tab_recv.at[zs],
            device_id={"sp": z + 1 if side else z - 1}, device_id_type=MESH,
        )

    def each_side(zs, act):
        @pl.when((zs <= z) & (z < n - 1))
        def _():
            act(1)

        @pl.when((zs >= z) & (z > 0))
        def _():
            act(0)

    each_side(z, lambda side: table_copy(z, side).start())

    for k in range(len(BANDS) - 1):
        piece = band(k)
        for i in range(1, q_count):
            spot = inc.at[base + i - 1, :, piece]
            pltpu.make_async_copy(spot, spot, part_recv.at[i - 1, k]).wait()
        square = jnp.zeros((piece.size, 1), jnp.float32)
        for c in range(PARTS):
            total = acc[c, piece] + kept[piece, col(c)].astype(jnp.float32)
            for i in range(1, q_count):
                total = total + inc[base + i - 1, c, piece].astype(jnp.float32)
            after = total.astype(jnp.bfloat16)
            kept[piece, col(c)] = after
            after = after.astype(jnp.float32)
            square = square + jnp.sum(after * after, axis=1, keepdims=True)
        norm = lax.rsqrt(square / width + 0.01)
        for c in range(PARTS):
            after = kept[piece, col(c)].astype(jnp.float32)
            toks[z, c, piece] = (after * norm * gain_ref[:, col(c)]).astype(jnp.bfloat16)
        each_side(z, lambda side: token_copy(z, k, side).start())


    upper = z > n - 1 - z
    middle = (z > 0) & (z < n - 1)

    def arrival(j):
        low = jnp.minimum(z, n - 1 - z)
        out = jnp.where(j <= 2 * low, (j + 1) // 2, j - low)
        down = jnp.where(j <= 2 * low, (j % 2 == 1) == upper, upper)
        return jnp.where(down, z - out, z + out)

    def source(i):
        mine = jnp.where(middle, 0, n - 1)
        return jnp.where(i == mine, z, arrival(jnp.where(middle, i, i + 1)))

    def span(index):
        return pl.ds(pl.multiple_of(index * cap, 16), cap)

    def exchange(j, c, to_ref, ss, rs):
        page = lax.rem(j, PAGES)
        for p in range(1, tp):
            other = lax.rem(t + p, tp)
            pltpu.make_async_remote_copy(
                src_ref=comp.at[page, c, span(other)],
                dst_ref=to_ref.at[page, c, span(t)],
                send_sem=ss.at[page],
                recv_sem=rs.at[page, c],
                device_id={"tp": other},
                device_id_type=MESH,
            ).start()
        to_ref[page, c, span(t)] = comp[page, c, span(t)]

    def wait_pieces(ref, page, c, rs):
        part = ref.at[page, c, pl.ds(0, (tp - 1) * cap)]
        pltpu.make_async_copy(part, part, rs.at[page, c]).wait()

    def wait_sent(page, ss):
        part = comp.at[page, :, pl.ds(0, (tp - 1) * cap)]
        pltpu.make_async_copy(part, part, ss.at[page]).wait()

    def piece_of(h):
        return pl.ds(h * (rows // SPLIT), rows // SPLIT)

    def sum_copy(zs, c, h, side):
        target = z + 1 if side else z - 1
        slot = jnp.where(target == zs, n, zs) if side else zs
        return pltpu.make_async_remote_copy(
            src_ref=toks.at[zs, c, piece_of(h)],
            dst_ref=inc.at[slot, c, piece_of(h)],
            send_sem=sum_send.at[zs],
            recv_sem=sum_recv.at[slot, c, h],
            device_id={"sp": target},
            device_id_type=MESH,
        )

    def names(zs):
        table = tabs[zs]
        start = (z * slots).astype(jnp.float32)
        place = lax.broadcasted_iota(jnp.int32, (slots, rows), 0).astype(jnp.float32) + start
        return place == table[0:1, :], place == table[1:2, :], table

    def passes_on(zs):
        return ((zs < z) & (z < n - 1)) | ((zs > z) & (z > 0))

    def arrive(zs, k):
        spot = toks.at[zs, :, band(k)]
        pltpu.make_async_copy(spot, spot, tok_recv.at[zs, k]).wait()

    def wait_passed(zs, side):
        table_copy(zs, side).wait_send()
        pltpu.make_async_copy(toks.at[zs], toks.at[zs], tok_send.at[side, zs]).wait()

    def hand_on(j):
        zs = arrival(jnp.minimum(j + 1, n - 1))

        @pl.when((j < n - 1) & passes_on(zs))
        def _():
            each_side(zs, lambda side: wait_passed(jnp.where(zs < z, zs + 1, zs - 1), side))
            pltpu.make_async_copy(tabs.at[zs], tabs.at[zs], tab_recv.at[zs]).wait()
            each_side(zs, lambda side: table_copy(zs, side).start())
            for k in range(len(BANDS) - 1):
                arrive(zs, k)
                each_side(zs, lambda side: token_copy(zs, k, side).start())

    def take(j):
        zs = source(j)

        @pl.when((zs != z) & jnp.logical_not(passes_on(zs)))
        def _():
            pltpu.make_async_copy(tabs.at[zs], tabs.at[zs], tab_recv.at[zs]).wait()
            for k in range(len(BANDS) - 1):
                arrive(zs, k)

        first, second, _ = names(zs)
        pick = jnp.where(first | second, 1.0, 0.0).astype(jnp.bfloat16)
        page = lax.rem(j, PAGES)
        for c in range(PARTS):
            comp[page, c] = jnp.dot(
                pick, toks[zs, c], preferred_element_type=jnp.float32
            ).astype(jnp.bfloat16)
            exchange(j, c, arr, piece_send, piece_recv)

    def run(j):
        page = lax.rem(j, PAGES)

        @pl.when(j == 0)
        def _():
            for load in expert_loads:
                load.wait()

        step = 256
        for c in range(PARTS):
            wait_pieces(arr, page, c, piece_recv)
            for f in range(0, hidden_width, step):
                for to, weights in ((ga, wg), (ua, wu)):
                    value = jnp.dot(
                        arr[page, c], weights[col(c), f : f + step],
                        preferred_element_type=jnp.float32,
                    )
                    if c:
                        value = value + to[:, f : f + step]
                    if c < PARTS - 1 or to is ga:
                        to[:, f : f + step] = value
                if c == PARTS - 1:
                    gate = ga[:, f : f + step]
                    hid[:, f : f + step] = (jax.nn.silu(gate) * value).astype(jnp.bfloat16)
        wait_sent(page, piece_send)
        for c in range(PARTS):
            comp[page, c] = jnp.dot(
                hid[...], wd[:, col(c)], preferred_element_type=jnp.float32
            ).astype(jnp.bfloat16)
            exchange(j, c, back, back_send, back_recv)

    def merge(j, after_part):
        zs = source(j)
        page = lax.rem(j, PAGES)
        first, second, table = names(zs)
        share = jnp.where(first, table[2:3, :], 0.0) + jnp.where(second, table[3:4, :], 0.0)
        share = share.T
        high = share.astype(jnp.bfloat16)
        rest = (share - high.astype(jnp.float32)).astype(jnp.bfloat16)

        def sent(side):
            @pl.when(zs == (0 if side else n - 1))
            def _():
                wait_passed(zs, side)

        each_side(zs, sent)
        for c in range(PARTS):
            wait_pieces(back, page, c, back_recv)
            value = jnp.dot(high, back[page, c], preferred_element_type=jnp.float32) + jnp.dot(
                rest, back[page, c], preferred_element_type=jnp.float32
            )

            @pl.when(zs == z)
            def _():
                acc[c] = value

            @pl.when(zs != z)
            def _():
                toks[zs, c] = value.astype(jnp.bfloat16)

            after_part(zs, c)
        wait_sent(page, back_send)

    def send_sums(zs, c):
        for side in range(2):
            @pl.when((zs > z) & (z == 0) if side else (zs < z) & (z == n - 1))
            def _():
                for h in range(SPLIT):
                    sum_copy(zs, c, h, side).start()

    def relay(turn, p, side):
        zs = turn if side else n - 1 - turn
        c, h = p // SPLIT, p % SPLIT

        @pl.when((z > 0) & (z < turn) if side else (z < n - 1) & (z > n - 1 - turn))
        def _():
            spot = inc.at[zs, c, piece_of(h)]
            pltpu.make_async_copy(spot, spot, sum_recv.at[zs, c, h]).wait()
            toks[zs, c, piece_of(h)] = (
                toks[zs, c, piece_of(h)].astype(jnp.float32)
                + inc[zs, c, piece_of(h)].astype(jnp.float32)
            ).astype(jnp.bfloat16)
            sum_copy(zs, c, h, side).start()

    def relays(turn, start, stop):
        def both(side):
            for p in range(start, stop):
                if p < PARTS * SPLIT:
                    relay(turn, p, side)
                if p >= LAG:
                    relay(turn, p - LAG, 1 - side)

        @pl.when((turn > 0) & upper)
        def _():
            both(0)

        @pl.when((turn > 0) & jnp.logical_not(upper))
        def _():
            both(1)

    def merge_and_relay(j):
        merge(j, lambda zs, c: relays(j, c * SPLIT, (c + 1) * SPLIT))
        relays(j, PARTS * SPLIT, PARTS * SPLIT + LAG)

    def body(j, carry):
        hand_on(j + 1)
        ahead = jnp.where(middle, j + 1, j)

        @pl.when(ahead < n)
        def _():
            take(ahead)

        @pl.when((j > 0) & jnp.logical_not(middle))
        def _():
            merge(j - 1, send_sums)

        @pl.when(j < n)
        def _():
            run(j)

        @pl.when((j > 0) & middle)
        def _():
            merge_and_relay(j - 1)

        return carry

    @pl.when(middle)
    def _():
        take(0)
        hand_on(0)

    lax.fori_loop(0, n + 1, body, 0)

    def final(c, h):
        piece = piece_of(h)

        @pl.when(z < n - 1)
        def _():
            spot = inc.at[z, c, piece]
            pltpu.make_async_copy(spot, spot, sum_recv.at[z, c, h]).wait()
            acc[c, piece] = acc[c, piece] + inc[z, c, piece].astype(jnp.float32)

        @pl.when(z > 0)
        def _():
            spot = inc.at[n, c, piece]
            pltpu.make_async_copy(spot, spot, sum_recv.at[n, c, h]).wait()
            acc[c, piece] = acc[c, piece] + inc[n, c, piece].astype(jnp.float32)

        kept[piece, col(c)] = (
            kept[piece, col(c)].astype(jnp.float32) + acc[c, piece]
        ).astype(jnp.bfloat16)
        pltpu.make_async_copy(
            kept.at[piece, col(c)], out_hbm.at[piece, col(c)], out_sem.at[0]
        ).start()

    for c in range(PARTS):
        for h in range(SPLIT):
            final(c, h)

    def drain(zs, carry):
        @pl.when(zs != z)
        def _():
            pltpu.make_async_copy(toks.at[zs], toks.at[zs], sum_send.at[zs]).wait()

        return carry

    lax.fori_loop(0, n, drain, 0)
    pltpu.make_async_copy(kept, out_hbm, out_sem.at[0]).wait()
    pltpu.make_async_copy(others, others, stat_send.at[0]).wait()
    for i in order:
        act_copy(i).wait_send()
        if i:
            spot = psend.at[i - 1]
            pltpu.make_async_copy(spot, spot, part_send.at[i - 1]).wait()

    @pl.when(z < n - 1)
    def _():
        halo_copy(1).wait_send()

    @pl.when(z > 0)
    def _():
        halo_copy(0).wait_send()


def shards(
    latents,
    conv_value,
    conv_gate,
    conv_taps,
    conv_gain,
    point_weight,
    channel_gain,
    expert_ids,
    expert_weights,
    gate_weight,
    up_weight,
    down_weight,
):
    n, tp = lax.axis_size("sp"), lax.axis_size("tp")
    rows, top_count = expert_ids.shape
    experts = gate_weight.shape[0] * n * tp
    cap = -(-(2 * top_count * rows // experts) // 16) * 16
    block, chans = conv_value.shape
    width = latents.shape[1]
    taps_count = conv_taps.shape[0]
    hidden_width = gate_weight.shape[2]
    slots = tp * cap
    cols = width // PARTS
    edge = -(-(taps_count // 2) // 16) * 16
    q_count = tp // 2
    spots = max(n + 1, 2 * chans // rows + q_count - 1)
    dma = pltpu.SemaphoreType.DMA
    bf16, f32 = jnp.bfloat16, jnp.float32
    anywhere = pl.BlockSpec(memory_space=pl.ANY)
    vmem = pltpu.VMEM
    return pl.pallas_call(
        functools.partial(layer_kernel, n, tp, taps_count, cap),
        out_shape=jax.ShapeDtypeStruct((rows, width), bf16),
        in_specs=[anywhere] * 12,
        out_specs=anywhere,
        scratch_shapes=[
            vmem((block, chans), bf16),
            vmem((block, chans), bf16),
            vmem((taps_count, chans), f32),
            vmem((1, chans), f32),
            vmem((1, width), f32),
            vmem((top_count, rows), jnp.int32),
            vmem((top_count, rows), f32),
            vmem((rows, width), bf16),
            vmem((block + 2 * edge, chans), bf16),
            vmem((rows + 2 * edge, chans), f32),
            vmem((tp, rows, chans), f32),
            vmem((tp, tp, 8, rows), f32),
            vmem((q_count, rows, chans), bf16),
            vmem((q_count, 2, rows, chans), bf16),
            vmem((q_count - 1, PARTS, rows, cols), bf16),
            vmem((n, PARTS, rows, cols), bf16),
            vmem((n, 8, rows), f32),
            vmem((PAGES, PARTS, slots, cols), bf16),
            vmem((PAGES, PARTS, slots, cols), bf16),
            vmem((PAGES, PARTS, slots, cols), bf16),
            vmem((spots, PARTS, rows, cols), bf16),
            vmem((PARTS, rows, cols), f32),
            vmem((width, hidden_width), bf16),
            vmem((width, hidden_width), bf16),
            vmem((hidden_width, width), bf16),
            vmem((slots, hidden_width), f32),
            vmem((slots, hidden_width), f32),
            vmem((slots, hidden_width), bf16),
            dma((8,)),
            dma((1,)),
            dma((3,)),
            dma((1,)),
            dma((2,)),
            dma((2,)),
            dma((1,)),
            dma((1,)),
            dma((1,)),
            dma((1,)),
            dma((q_count,)),
            dma((q_count,)),
            dma((q_count - 1,)),
            dma((q_count - 1, len(BANDS) - 1)),
            dma((2, n)),
            dma((n, len(BANDS) - 1)),
            dma((2, n)),
            dma((n,)),
            dma((PAGES,)),
            dma((PAGES, PARTS)),
            dma((PAGES,)),
            dma((PAGES, PARTS)),
            dma((n,)),
            dma((n + 1, PARTS, SPLIT)),
        ],
        compiler_params=pltpu.CompilerParams(
            collective_id=0, has_side_effects=True, vmem_limit_bytes=67043328
        ),
        name="layer",
    )(
        conv_value, conv_gate, conv_taps, conv_gain[None, :], point_weight, latents,
        channel_gain[None, :], expert_ids.T, expert_weights.T,
        gate_weight, up_weight, down_weight,
    )


def solution(mesh):
    return jax.shard_map(
        shards,
        mesh=mesh,
        in_specs=(
            P(("grp", "sp", "tp"), None),
            P(("grp", "sp"), "tp"),
            P(("grp", "sp"), "tp"),
            P(None, "tp"),
            P("tp"),
            P("tp", None),
            P(),
            P(("grp", "sp", "tp"), None),
            P(("grp", "sp", "tp"), None),
            P(("sp", "tp"), None, None),
            P(("sp", "tp"), None, None),
            P(("sp", "tp"), None, None),
        ),
        out_specs=P(("grp", "sp", "tp"), None),
        check_vma=False,
    )
```

```python
import functools

import jax
import jax.numpy as jnp
from jax import lax
from jax.experimental import pallas as pl
from jax.experimental.pallas import tpu as pltpu
from jax.sharding import PartitionSpec as P


MESH = pl.DeviceIdType.MESH
PARTS = 4
BANDS = (0, 1, 2, 3, 4, 5, 6, 7, 8)
SPLIT = 2
LAG = 3
PAGES = 3


def layer_kernel(
    n, tp, taps_count, cap,
    value_hbm, gate_hbm, taps_hbm, cgain_hbm, weight_hbm, latent_hbm, gain_hbm, ids_hbm, share_hbm,
    wg_hbm, wu_hbm, wd_hbm, out_hbm,
    value_ref, gate_ref, taps_ref, cgain_ref, gain_ref, ids_ref, share_ref,
    kept, gated, wide, mixed, stats, act_out, act_in, psend,
    toks, tabs, comp, outs, arr, back, inc, acc, wg, wu, wd, ga, ua, hid,
    load_sem, point_sem, w_sem, out_sem, halo_send, halo_recv, stat_send, stat_recv, mate_send, mate_recv,
    act_send, act_recv, part_send, part_recv,
    tok_send, tok_recv, tab_send, tab_recv,
    piece_send, piece_recv, back_send, back_recv, sum_send, sum_recv, turn_sem,
):
    z = lax.axis_index("sp")
    t = lax.axis_index("tp")
    block, chans = value_ref.shape
    rows, width = kept.shape
    slots = tp * cap
    groups = 2 if cap % 32 == 0 else 1
    depth = cap // groups
    group_rows = slots // groups
    hidden_width = wg.shape[1]
    top_count = ids_ref.shape[0]
    cols = width // PARTS
    half = taps_count // 2
    edge = (gated.shape[0] - block) // 2
    view = rows // 2 + 2 * edge
    q_count = tp // 2
    core = lax.rem(t, 2)
    quad = t // 2
    mate = t + 1 - 2 * core
    chunks = chans // rows
    base = 2 * chunks

    def band(k):
        return pl.ds(BANDS[k] * rows // BANDS[-1], (BANDS[k + 1] - BANDS[k]) * rows // BANDS[-1])

    def col(c):
        return pl.ds(c * cols, cols)

    loads = [
        pltpu.make_async_copy(a, b, load_sem.at[i])
        for i, (a, b) in enumerate(
            (
                (value_hbm, value_ref),
                (gate_hbm, gate_ref),
                (taps_hbm, taps_ref),
                (cgain_hbm, cgain_ref),
                (ids_hbm, ids_ref),
                (share_hbm, share_ref),
                (gain_hbm, gain_ref),
                (latent_hbm, kept),
            )
        )
    ]
    for load in loads:
        load.start()

    point_loads = [
        pltpu.make_async_copy(
            weight_hbm.at[pl.ds(b * rows, rows), col(c)],
            inc.at[core * chunks + b, c],
            point_sem.at[0],
        )
        for b in range(chunks)
        for c in range(PARTS)
    ]
    for load in point_loads:
        load.start()

    barrier = pltpu.get_barrier_semaphore()
    for p in range(1, tp):
        pl.semaphore_signal(
            barrier, inc=1, device_id={"tp": lax.rem(t + p, tp)}, device_id_type=MESH
        )

    @pl.when(z > 0)
    def _():
        pl.semaphore_signal(barrier, inc=1, device_id={"sp": z - 1}, device_id_type=MESH)

    @pl.when(z < n - 1)
    def _():
        pl.semaphore_signal(barrier, inc=1, device_id={"sp": z + 1}, device_id_type=MESH)

    @pl.when(z == 0)
    def _():
        gated[pl.ds(0, edge)] = jnp.zeros((edge, chans), jnp.bfloat16)

    @pl.when(z == n - 1)
    def _():
        gated[pl.ds(edge + block, edge)] = jnp.zeros((edge, chans), jnp.bfloat16)

    loads[0].wait()
    loads[1].wait()
    step = 64
    for r in range(0, block, step):
        value = value_ref[pl.ds(r, step)].astype(jnp.float32)
        gate = gate_ref[pl.ds(r, step)].astype(jnp.float32)
        gated[pl.ds(edge + r, step)] = (value * jax.nn.sigmoid(gate)).astype(jnp.bfloat16)

    peers = tp - 1 + (z > 0).astype(jnp.int32) + (z < n - 1).astype(jnp.int32)
    pl.semaphore_wait(barrier, peers)

    def halo_copy(up):
        start = block if up else edge
        place = 0 if up else edge + block
        return pltpu.make_async_remote_copy(
            src_ref=gated.at[pl.ds(start, edge)], dst_ref=gated.at[pl.ds(place, edge)],
            send_sem=halo_send.at[up], recv_sem=halo_recv.at[up],
            device_id={"sp": z + 1 if up else z - 1}, device_id_type=MESH,
        )

    @pl.when(z < n - 1)
    def _():
        halo_copy(1).start()

    @pl.when(z > 0)
    def _():
        halo_copy(0).start()

    own_rows = pl.ds(core * chunks, chunks)
    pltpu.make_async_copy(inc.at[own_rows], inc.at[own_rows], point_sem.at[0]).wait()
    mate_copy = pltpu.make_async_remote_copy(
        src_ref=inc.at[own_rows], dst_ref=inc.at[own_rows],
        send_sem=mate_send.at[0], recv_sem=mate_recv.at[0],
        device_id={"tp": mate}, device_id_type=MESH,
    )
    mate_copy.start()

    expert_loads = [
        pltpu.make_async_copy(a, b, w_sem.at[i])
        for i, (a, b) in enumerate(((wg_hbm.at[0], wg), (wu_hbm.at[0], wu), (wd_hbm.at[0], wd)))
    ]
    for load in loads[2:]:
        load.wait()

    tile = rows // 2

    def convolve(s, r):
        start = pl.multiple_of(s * rows + r, 16)
        wide[0] = gated[pl.ds(start, view)].astype(jnp.float32)
        for b in range(1, 8):
            wide[b, pl.ds(0, view - 8)] = wide[0, pl.ds(b, view - 8)]
        value = jnp.zeros((tile, chans), jnp.float32)
        for i in range(taps_count):
            a, b = divmod(edge - half + i, 8)
            value = value + taps_ref[pl.ds(i, 1)] * wide[b, pl.ds(8 * a, tile)]
        mixed[s, pl.ds(pl.multiple_of(r, 16), tile)] = value

    def measure(s):
        value = mixed[s]
        for k, summed in enumerate((value, value * value)):
            line = jnp.broadcast_to(jnp.sum(summed, axis=1, keepdims=True), (rows, rows)).T
            stats[t, s, pl.ds(k, 1)] = line[0:1]
        for p in range(1, tp):
            pltpu.make_async_remote_copy(
                src_ref=stats.at[t, s], dst_ref=stats.at[t, s],
                send_sem=stat_send.at[0], recv_sem=stat_recv.at[s],
                device_id={"tp": lax.rem(t + p, tp)}, device_id_type=MESH,
            ).start()

    def inner(i, carry):
        s = jnp.where(quad == 0, tp - 2 - i, i + 1)
        convolve(s, 0)
        convolve(s, tile)
        measure(s)
        return carry

    def near_edge(i, carry):
        convolve(i * (tp - 1), (1 - i) * tile)
        return carry

    def at_edge(i, carry):
        side = jnp.where(quad == 0, 1 - i, i)
        convolve(side * (tp - 1), side * tile)
        measure(side * (tp - 1))
        return carry

    lax.fori_loop(0, tp - 2, inner, 0)
    lax.fori_loop(0, 2, near_edge, 0)

    @pl.when(z > 0)
    def _():
        halo_copy(1).wait_recv()

    @pl.when(z < n - 1)
    def _():
        halo_copy(0).wait_recv()

    lax.fori_loop(0, 2, at_edge, 0)
    for load in expert_loads:
        load.start()

    ids = ids_ref[...].astype(jnp.float32)
    across = [jnp.broadcast_to(ids[k : k + 1], (rows, rows)) for k in range(top_count)]
    down = [value.T for value in across]
    down_place = lax.broadcasted_iota(jnp.int32, (rows, rows), 0)
    across_place = lax.broadcasted_iota(jnp.int32, (rows, rows), 1)
    tabs[z] = jnp.zeros(tabs.shape[1:], jnp.float32)
    for k in range(top_count):
        count = jnp.zeros((1, rows), jnp.float32)
        for m in range(k + 1):
            same = down[m] == across[k]
            if m == k:
                same = same & (down_place < across_place)
            count = count + jnp.sum(jnp.where(same, 1.0, 0.0), axis=0, keepdims=True)
        tabs[z, pl.ds(k, 1)] = ids[k : k + 1] * cap + count
        tabs[z, pl.ds(top_count + k, 1)] = share_ref[pl.ds(k, 1)]

    def activate_block(s):
        others = stats.at[pl.ds(0, tp - 1), s]
        pltpu.make_async_copy(others, others, stat_recv.at[s]).wait()
        both = stats[0, s]
        for p in range(1, tp):
            both = both + stats[p, s]
        both = both / (chans * tp)
        center = both[0:1]
        scale = lax.rsqrt(both[1:2] - center * center + 0.05)
        center = jnp.broadcast_to(center, (rows, rows)).T[:, 0:1]
        scale = jnp.broadcast_to(scale, (rows, rows)).T[:, 0:1]
        value = (mixed[s] - center) * scale * cgain_ref[...]
        return jax.nn.silu(value).astype(jnp.bfloat16)

    def spot_of(e, which):
        return jnp.where(which == 0, (e + 1) % q_count, e)

    def act_copy(spot):
        return pltpu.make_async_remote_copy(
            src_ref=act_out.at[spot], dst_ref=act_in.at[spot, core],
            send_sem=act_send.at[spot], recv_sem=act_recv.at[spot],
            device_id={"tp": mate}, device_id_type=MESH,
        )

    def product(spot, c):
        left = jnp.concatenate([act_in[spot, 0], act_in[spot, 1]], axis=1)
        right = inc[pl.ds(0, base), c].reshape(base * rows, cols)
        return jnp.dot(left, right, preferred_element_type=jnp.float32)

    def part_copy(spot, k):
        i = lax.rem(spot - quad + q_count, q_count) - 1
        piece = band(k)
        return pltpu.make_async_remote_copy(
            src_ref=psend.at[i, :, piece], dst_ref=inc.at[base + i, :, piece],
            send_sem=part_send.at[i], recv_sem=part_recv.at[i, k],
            device_id={"tp": 2 * spot + core}, device_id_type=MESH,
        )

    for e in range(q_count):
        theirs, ours = spot_of(e, 1 - core), spot_of(e, core)
        act_out[theirs] = activate_block(2 * theirs + 1 - core)
        act_copy(theirs).start()
        act_in[ours, core] = activate_block(2 * ours + core)
        if e == 0:
            mate_copy.wait()
        pltpu.make_async_copy(act_out.at[ours], act_out.at[ours], act_recv.at[ours]).wait()

        @pl.when(ours != quad)
        def _():
            i = lax.rem(ours - quad + q_count, q_count) - 1
            for c in range(PARTS):
                psend[i, c] = product(ours, c).astype(jnp.bfloat16)
            for k in range(len(BANDS) - 1):
                part_copy(ours, k).start()

        @pl.when(ours == quad)
        def _():
            for c in range(PARTS):
                acc[c] = product(ours, c)

    def token_copy(zs, k, side):
        piece = band(k)
        return pltpu.make_async_remote_copy(
            src_ref=toks.at[zs, :, piece], dst_ref=toks.at[zs, :, piece],
            send_sem=tok_send.at[side, zs], recv_sem=tok_recv.at[zs, k],
            device_id={"sp": z + 1 if side else z - 1}, device_id_type=MESH,
        )

    def table_copy(zs, side):
        return pltpu.make_async_remote_copy(
            src_ref=tabs.at[zs], dst_ref=tabs.at[zs],
            send_sem=tab_send.at[side, zs], recv_sem=tab_recv.at[zs],
            device_id={"sp": z + 1 if side else z - 1}, device_id_type=MESH,
        )

    def each_side(zs, act):
        @pl.when((zs <= z) & (z < n - 1))
        def _():
            act(1)

        @pl.when((zs >= z) & (z > 0))
        def _():
            act(0)

    each_side(z, lambda side: table_copy(z, side).start())

    for k in range(len(BANDS) - 1):
        piece = band(k)
        for i in range(1, q_count):
            spot = inc.at[base + i - 1, :, piece]
            pltpu.make_async_copy(spot, spot, part_recv.at[i - 1, k]).wait()
        square = jnp.zeros((piece.size, 1), jnp.float32)
        for c in range(PARTS):
            total = acc[c, piece] + kept[piece, col(c)].astype(jnp.float32)
            for i in range(1, q_count):
                total = total + inc[base + i - 1, c, piece].astype(jnp.float32)
            after = total.astype(jnp.bfloat16)
            kept[piece, col(c)] = after
            after = after.astype(jnp.float32)
            square = square + jnp.sum(after * after, axis=1, keepdims=True)
        norm = lax.rsqrt(square / width + 0.01)
        for c in range(PARTS):
            after = kept[piece, col(c)].astype(jnp.float32)
            toks[z, c, piece] = (after * norm * gain_ref[:, col(c)]).astype(jnp.bfloat16)
        each_side(z, lambda side: token_copy(z, k, side).start())


    upper = z > n - 1 - z
    middle = (z > 0) & (z < n - 1)

    def arrival(j):
        low = jnp.minimum(z, n - 1 - z)
        out = jnp.where(j <= 2 * low, (j + 1) // 2, j - low)
        down = jnp.where(j <= 2 * low, (j % 2 == 1) == upper, upper)
        return jnp.where(down, z - out, z + out)

    def source(i):
        mine = jnp.where(middle, 0, n - 1)
        return jnp.where(i == mine, z, arrival(jnp.where(middle, i, i + 1)))

    def span(g, index):
        return pl.ds(pl.multiple_of(g * group_rows + index * depth, 16), depth)

    def group(g):
        return pl.ds(g * group_rows, group_rows)

    def exchange(j, g, c, from_ref, to_ref, ss, rs):
        page = lax.rem(j, PAGES)
        side = lax.rem(j, 2)
        for p in range(1, tp):
            other = lax.rem(t + p, tp)
            pltpu.make_async_remote_copy(
                src_ref=from_ref.at[side, c, span(g, other)],
                dst_ref=to_ref.at[page, c, span(g, t)],
                send_sem=ss.at[side],
                recv_sem=rs.at[page, g, c],
                device_id={"tp": other},
                device_id_type=MESH,
            ).start()
        to_ref[page, c, span(g, t)] = from_ref[side, c, span(g, t)]

    def wait_pieces(ref, page, g, c, rs):
        part = ref.at[page, c, pl.ds(0, (tp - 1) * depth)]
        pltpu.make_async_copy(part, part, rs.at[page, g, c]).wait()

    def wait_sent(j, from_ref, ss):
        part = from_ref.at[lax.rem(j, 2), :, pl.ds(0, (tp - 1) * cap)]
        pltpu.make_async_copy(part, part, ss.at[lax.rem(j, 2)]).wait()

    def piece_of(h):
        return pl.ds(h * (rows // SPLIT), rows // SPLIT)

    def sum_copy(zs, c, h, side):
        target = z + 1 if side else z - 1
        slot = jnp.where(target == zs, n, zs) if side else zs
        return pltpu.make_async_remote_copy(
            src_ref=toks.at[zs, c, piece_of(h)],
            dst_ref=inc.at[slot, c, piece_of(h)],
            send_sem=sum_send.at[zs],
            recv_sem=sum_recv.at[slot, c, h],
            device_id={"sp": target},
            device_id_type=MESH,
        )

    def names(zs):
        table = tabs[zs]
        start = (z * slots).astype(jnp.float32)
        row = lax.broadcasted_iota(jnp.int32, (slots, rows), 0)
        place = (
            lax.rem(row, group_rows) // depth * cap + row // group_rows * depth + lax.rem(row, depth)
        )
        place = place.astype(jnp.float32) + start
        return place == table[0:1, :], place == table[1:2, :], table

    def passes_on(zs):
        return ((zs < z) & (z < n - 1)) | ((zs > z) & (z > 0))

    def arrive(zs, k):
        spot = toks.at[zs, :, band(k)]
        pltpu.make_async_copy(spot, spot, tok_recv.at[zs, k]).wait()

    def wait_passed(zs, side):
        table_copy(zs, side).wait_send()
        pltpu.make_async_copy(toks.at[zs], toks.at[zs], tok_send.at[side, zs]).wait()

    def hand_on(j):
        zs = arrival(jnp.minimum(j + 1, n - 1))

        @pl.when((j < n - 1) & passes_on(zs))
        def _():
            previous = jnp.where(zs < z, zs + 1, zs - 1)

            @pl.when(previous != z)
            def _():
                each_side(zs, lambda side: wait_passed(previous, side))

            pltpu.make_async_copy(tabs.at[zs], tabs.at[zs], tab_recv.at[zs]).wait()
            each_side(zs, lambda side: table_copy(zs, side).start())
            for k in range(len(BANDS) - 1):
                arrive(zs, k)
                each_side(zs, lambda side: token_copy(zs, k, side).start())

    def take(j):
        zs = source(j)

        @pl.when((zs != z) & jnp.logical_not(passes_on(zs)))
        def _():
            pltpu.make_async_copy(tabs.at[zs], tabs.at[zs], tab_recv.at[zs]).wait()
            for k in range(len(BANDS) - 1):
                arrive(zs, k)

        first, second, _ = names(zs)
        pick = jnp.where(first | second, 1.0, 0.0).astype(jnp.bfloat16)
        side = lax.rem(j, 2)
        for c in range(PARTS):
            comp[side, c] = jnp.dot(
                pick, toks[zs, c], preferred_element_type=jnp.float32
            ).astype(jnp.bfloat16)
            exchange(j, 0, c, comp, arr, piece_send, piece_recv)
        for g in range(1, groups):
            for c in range(PARTS):
                exchange(j, g, c, comp, arr, piece_send, piece_recv)

    def run(j, after_group):
        page = lax.rem(j, PAGES)
        side = lax.rem(j, 2)

        @pl.when(j == 0)
        def _():
            for load in expert_loads:
                load.wait()

        step = 256
        for g in range(groups):
            for c in range(PARTS):
                wait_pieces(arr, page, g, c, piece_recv)
                for f in range(0, hidden_width, step):
                    for to, weights in ((ga, wg), (ua, wu)):
                        value = jnp.dot(
                            arr[page, c, group(g)], weights[col(c), f : f + step],
                            preferred_element_type=jnp.float32,
                        )
                        if c:
                            value = value + to[:, f : f + step]
                        if c < PARTS - 1 or to is ga:
                            to[:, f : f + step] = value
                    if c == PARTS - 1:
                        gate = ga[:, f : f + step]
                        hid[:, f : f + step] = (jax.nn.silu(gate) * value).astype(jnp.bfloat16)
            for c in range(PARTS):
                outs[side, c, group(g)] = jnp.dot(
                    hid[...], wd[:, col(c)], preferred_element_type=jnp.float32
                ).astype(jnp.bfloat16)
                exchange(j, g, c, outs, back, back_send, back_recv)
            after_group(g)
        wait_sent(j, comp, piece_send)

    def merge(j, after_part):
        zs = source(j)
        page = lax.rem(j, PAGES)
        first, second, table = names(zs)
        share = jnp.where(first, table[2:3, :], 0.0) + jnp.where(second, table[3:4, :], 0.0)
        share = share.T
        high = share.astype(jnp.bfloat16)
        rest = (share - high.astype(jnp.float32)).astype(jnp.bfloat16)

        def sent(side):
            @pl.when((zs == (0 if side else n - 1)) & ((zs != z) | jnp.logical_not(middle)))
            def _():
                wait_passed(zs, side)

        each_side(zs, sent)
        for c in range(PARTS):
            for g in range(groups):
                wait_pieces(back, page, g, c, back_recv)
            value = jnp.dot(high, back[page, c], preferred_element_type=jnp.float32) + jnp.dot(
                rest, back[page, c], preferred_element_type=jnp.float32
            )

            @pl.when(zs == z)
            def _():
                acc[c] = value

            @pl.when(zs != z)
            def _():
                toks[zs, c] = value.astype(jnp.bfloat16)

            after_part(zs, c)
        wait_sent(j, outs, back_send)

    def send_sums(zs, c):
        for side in range(2):
            @pl.when((zs > z) & (z == 0) if side else (zs < z) & (z == n - 1))
            def _():
                for h in range(SPLIT):
                    sum_copy(zs, c, h, side).start()

    def relay(turn, p, side):
        zs = turn if side else n - 1 - turn
        c, h = p // SPLIT, p % SPLIT

        @pl.when((z > 0) & (z < turn) if side else (z < n - 1) & (z > n - 1 - turn))
        def _():
            spot = inc.at[zs, c, piece_of(h)]
            pltpu.make_async_copy(spot, spot, sum_recv.at[zs, c, h]).wait()
            toks[zs, c, piece_of(h)] = (
                toks[zs, c, piece_of(h)].astype(jnp.float32)
                + inc[zs, c, piece_of(h)].astype(jnp.float32)
            ).astype(jnp.bfloat16)
            sum_copy(zs, c, h, side).start()

    def relays(turn, start, stop):
        def both(side):
            for p in range(start, stop):
                if p < PARTS * SPLIT:
                    relay(turn, p, side)
                if p >= LAG:
                    relay(turn, p - LAG, 1 - side)

        @pl.when((turn > 0) & upper)
        def _():
            both(0)

        @pl.when((turn > 0) & jnp.logical_not(upper))
        def _():
            both(1)

    def merged(zs, j):
        out = jnp.abs(zs - z)
        low = jnp.minimum(z, n - 1 - z)
        near = jnp.where((zs < z) == upper, 2 * out - 1, 2 * out)
        return jnp.where(out <= low, near, out + low) < j

    def is_early(turn):
        up = (z >= turn) | merged(turn, turn)
        down = (z <= n - 1 - turn) | merged(n - 1 - turn, turn)
        return middle & (turn > 0) & up & down

    pieces = PARTS * SPLIT
    early_stops = (pieces // 4, pieces // 2 + 1, pieces + LAG)

    def early_relays(turn, stop):
        start = (0,) + early_stops
        start = start[start.index(stop) - 1]

        @pl.when(is_early(turn))
        def _():
            relays(turn, start, stop)

    def merge_and_relay(j):
        late = jnp.logical_not(is_early(j))

        def after(zs, c):
            @pl.when(late)
            def _():
                relays(j, c * SPLIT, (c + 1) * SPLIT)

        merge(j, after)

        @pl.when(late)
        def _():
            relays(j, pieces, pieces + LAG)

    def body(j, carry):
        ahead = jnp.where(middle, j + 1, j)

        @pl.when((j == 1) & jnp.logical_not(middle))
        def _():
            merge(j - 1, send_sums)

        @pl.when(ahead < n)
        def _():
            take(ahead)

        @pl.when((j > 1) & jnp.logical_not(middle))
        def _():
            merge(j - 1, send_sums)

        @pl.when(j < n)
        def _():
            early_relays(j - 1, early_stops[0])
            run(j, lambda g: early_relays(j - 1, early_stops[min(g + 1, 1)]) if g == 0 else None)
            early_relays(j - 1, early_stops[2])

        @pl.when(j > 0)
        def _():
            hand_on(j + 1)

        @pl.when((j > 0) & middle)
        def _():
            merge_and_relay(j - 1)

        return carry

    @pl.when(middle)
    def _():
        take(0)
        each_side(z, lambda side: wait_passed(z, side))
        pl.semaphore_signal(turn_sem, inc=1, device_id={"tp": mate}, device_id_type=MESH)
        pl.semaphore_wait(turn_sem, 1)
        hand_on(0)
        hand_on(1)

    lax.fori_loop(0, n + 1, body, 0)

    def final(c, h):
        piece = piece_of(h)

        @pl.when(z < n - 1)
        def _():
            spot = inc.at[z, c, piece]
            pltpu.make_async_copy(spot, spot, sum_recv.at[z, c, h]).wait()
            acc[c, piece] = acc[c, piece] + inc[z, c, piece].astype(jnp.float32)

        @pl.when(z > 0)
        def _():
            spot = inc.at[n, c, piece]
            pltpu.make_async_copy(spot, spot, sum_recv.at[n, c, h]).wait()
            acc[c, piece] = acc[c, piece] + inc[n, c, piece].astype(jnp.float32)

        kept[piece, col(c)] = (
            kept[piece, col(c)].astype(jnp.float32) + acc[c, piece]
        ).astype(jnp.bfloat16)
        pltpu.make_async_copy(
            kept.at[piece, col(c)], out_hbm.at[piece, col(c)], out_sem.at[0]
        ).start()

    for c in range(PARTS):
        for h in range(SPLIT):
            final(c, h)

    def drain(zs, carry):
        @pl.when(zs != z)
        def _():
            pltpu.make_async_copy(toks.at[zs], toks.at[zs], sum_send.at[zs]).wait()

        return carry

    lax.fori_loop(0, n, drain, 0)
    pltpu.make_async_copy(kept, out_hbm, out_sem.at[0]).wait()
    others = stats.at[pl.ds(0, tp - 1)]
    pltpu.make_async_copy(others, others, stat_send.at[0]).wait()
    for e in range(q_count):
        act_copy(e).wait_send()
    for i in range(q_count - 1):
        pltpu.make_async_copy(psend.at[i], psend.at[i], part_send.at[i]).wait()

    @pl.when(z < n - 1)
    def _():
        halo_copy(1).wait_send()

    @pl.when(z > 0)
    def _():
        halo_copy(0).wait_send()


def shards(
    latents,
    conv_value,
    conv_gate,
    conv_taps,
    conv_gain,
    point_weight,
    channel_gain,
    expert_ids,
    expert_weights,
    gate_weight,
    up_weight,
    down_weight,
):
    n, tp = lax.axis_size("sp"), lax.axis_size("tp")
    rows, top_count = expert_ids.shape
    experts = gate_weight.shape[0] * n * tp
    cap = -(-(2 * top_count * rows // experts) // 16) * 16
    block, chans = conv_value.shape
    width = latents.shape[1]
    taps_count = conv_taps.shape[0]
    hidden_width = gate_weight.shape[2]
    slots = tp * cap
    groups = 2 if cap % 32 == 0 else 1
    cols = width // PARTS
    edge = -(-(taps_count // 2) // 16) * 16
    q_count = tp // 2
    spots = max(n + 1, 2 * chans // rows + q_count - 1)
    dma = pltpu.SemaphoreType.DMA
    bf16, f32 = jnp.bfloat16, jnp.float32
    anywhere = pl.BlockSpec(memory_space=pl.ANY)
    vmem = pltpu.VMEM
    return pl.pallas_call(
        functools.partial(layer_kernel, n, tp, taps_count, cap),
        out_shape=jax.ShapeDtypeStruct((rows, width), bf16),
        in_specs=[anywhere] * 12,
        out_specs=anywhere,
        scratch_shapes=[
            vmem((block, chans), bf16),
            vmem((block, chans), bf16),
            vmem((taps_count, chans), f32),
            vmem((1, chans), f32),
            vmem((1, width), f32),
            vmem((top_count, rows), jnp.int32),
            vmem((top_count, rows), f32),
            vmem((rows, width), bf16),
            vmem((block + 2 * edge, chans), bf16),
            vmem((8, rows // 2 + 2 * edge, chans), f32),
            vmem((tp, rows, chans), f32),
            vmem((tp, tp, 8, rows), f32),
            vmem((q_count, rows, chans), bf16),
            vmem((q_count, 2, rows, chans), bf16),
            vmem((q_count - 1, PARTS, rows, cols), bf16),
            vmem((n, PARTS, rows, cols), bf16),
            vmem((n, 8, rows), f32),
            vmem((2, PARTS, slots, cols), bf16),
            vmem((2, PARTS, slots, cols), bf16),
            vmem((PAGES, PARTS, slots, cols), bf16),
            vmem((PAGES, PARTS, slots, cols), bf16),
            vmem((spots, PARTS, rows, cols), bf16),
            vmem((PARTS, rows, cols), f32),
            vmem((width, hidden_width), bf16),
            vmem((width, hidden_width), bf16),
            vmem((hidden_width, width), bf16),
            vmem((slots // groups, hidden_width), f32),
            vmem((slots // groups, hidden_width), f32),
            vmem((slots // groups, hidden_width), bf16),
            dma((8,)),
            dma((1,)),
            dma((3,)),
            dma((1,)),
            dma((2,)),
            dma((2,)),
            dma((1,)),
            dma((tp,)),
            dma((1,)),
            dma((1,)),
            dma((q_count,)),
            dma((q_count,)),
            dma((q_count - 1,)),
            dma((q_count - 1, len(BANDS) - 1)),
            dma((2, n)),
            dma((n, len(BANDS) - 1)),
            dma((2, n)),
            dma((n,)),
            dma((2,)),
            dma((PAGES, groups, PARTS)),
            dma((2,)),
            dma((PAGES, groups, PARTS)),
            dma((n,)),
            dma((n + 1, PARTS, SPLIT)),
            pltpu.SemaphoreType.REGULAR,
        ],
        compiler_params=pltpu.CompilerParams(
            collective_id=0, has_side_effects=True, vmem_limit_bytes=67043328
        ),
        name="layer",
    )(
        conv_value, conv_gate, conv_taps, conv_gain[None, :], point_weight, latents,
        channel_gain[None, :], expert_ids.T, expert_weights.T,
        gate_weight, up_weight, down_weight,
    )


def solution(mesh):
    return jax.shard_map(
        shards,
        mesh=mesh,
        in_specs=(
            P(("grp", "sp", "tp"), None),
            P(("grp", "sp"), "tp"),
            P(("grp", "sp"), "tp"),
            P(None, "tp"),
            P("tp"),
            P("tp", None),
            P(),
            P(("grp", "sp", "tp"), None),
            P(("grp", "sp", "tp"), None),
            P(("sp", "tp"), None, None),
            P(("sp", "tp"), None, None),
            P(("sp", "tp"), None, None),
        ),
        out_specs=P(("grp", "sp", "tp"), None),
        check_vma=False,
    )
```

```python
import functools

import jax
import jax.numpy as jnp
from jax import lax
from jax.experimental import pallas as pl
from jax.experimental.pallas import tpu as pltpu
from jax.sharding import PartitionSpec as P


MESH = pl.DeviceIdType.MESH
PARTS = 4
BANDS = (0, 1, 2, 3, 4, 5, 6, 7, 8)
SPLIT = 4
LAG = 5
PAGES = 3


def layer_kernel(
    n, tp, taps_count, cap,
    value_hbm, gate_hbm, taps_hbm, cgain_hbm, weight_hbm, latent_hbm, gain_hbm, ids_hbm, share_hbm,
    wg_hbm, wu_hbm, wd_hbm, kept,
    value_ref, gate_ref, taps_ref, cgain_ref, gain_ref, ids_ref, share_ref,
    gated, wide, mixed, stats, act_out, act_in, psend,
    toks, tabs, comp, outs, arr, back, inc, acc, wg, wu, wd, ga, ua, hid,
    load_sem, point_sem, w_sem, halo_send, halo_recv, stat_send, stat_recv, mate_send, mate_recv,
    act_send, act_recv, part_send, part_recv,
    tok_send, tok_recv, tab_send, tab_recv,
    piece_send, piece_recv, back_send, back_recv, sum_send, sum_recv, turn_sem,
):
    z = lax.axis_index("sp")
    t = lax.axis_index("tp")
    block, chans = value_ref.shape
    rows, width = kept.shape
    slots = tp * cap
    groups = 2 if cap % 32 == 0 else 1
    depth = cap // groups
    group_rows = slots // groups
    hidden_width = wg.shape[1]
    top_count = ids_ref.shape[0]
    cols = width // PARTS
    half = taps_count // 2
    edge = (gated.shape[0] - block) // 2
    view = rows // 2 + 2 * edge
    q_count = tp // 2
    core = lax.rem(t, 2)
    quad = t // 2
    mate = t + 1 - 2 * core
    chunks = chans // rows
    base = 2 * chunks

    def band(k):
        return pl.ds(BANDS[k] * rows // BANDS[-1], (BANDS[k + 1] - BANDS[k]) * rows // BANDS[-1])

    def col(c):
        return pl.ds(c * cols, cols)

    loads = [
        pltpu.make_async_copy(a, b, load_sem.at[i])
        for i, (a, b) in enumerate(
            (
                (value_hbm, value_ref),
                (gate_hbm, gate_ref),
                (taps_hbm, taps_ref),
                (cgain_hbm, cgain_ref),
                (ids_hbm, ids_ref),
                (share_hbm, share_ref),
                (gain_hbm, gain_ref),
                (latent_hbm, kept),
            )
        )
    ]
    for load in loads:
        load.start()

    point_loads = [
        pltpu.make_async_copy(
            weight_hbm.at[pl.ds(b * rows, rows), col(c)],
            inc.at[core * chunks + b, c],
            point_sem.at[0],
        )
        for b in range(chunks)
        for c in range(PARTS)
    ]
    for load in point_loads:
        load.start()

    barrier = pltpu.get_barrier_semaphore()
    for p in range(1, tp):
        pl.semaphore_signal(
            barrier, inc=1, device_id={"tp": lax.rem(t + p, tp)}, device_id_type=MESH
        )

    @pl.when(z > 0)
    def _():
        pl.semaphore_signal(barrier, inc=1, device_id={"sp": z - 1}, device_id_type=MESH)

    @pl.when(z < n - 1)
    def _():
        pl.semaphore_signal(barrier, inc=1, device_id={"sp": z + 1}, device_id_type=MESH)

    @pl.when(z == 0)
    def _():
        gated[pl.ds(0, edge)] = jnp.zeros((edge, chans), jnp.bfloat16)

    @pl.when(z == n - 1)
    def _():
        gated[pl.ds(edge + block, edge)] = jnp.zeros((edge, chans), jnp.bfloat16)

    loads[0].wait()
    loads[1].wait()
    step = 64
    for r in range(0, block, step):
        value = value_ref[pl.ds(r, step)].astype(jnp.float32)
        gate = gate_ref[pl.ds(r, step)].astype(jnp.float32)
        gated[pl.ds(edge + r, step)] = (value * jax.nn.sigmoid(gate)).astype(jnp.bfloat16)

    peers = tp - 1 + (z > 0).astype(jnp.int32) + (z < n - 1).astype(jnp.int32)
    pl.semaphore_wait(barrier, peers)

    def halo_copy(up):
        start = block if up else edge
        place = 0 if up else edge + block
        return pltpu.make_async_remote_copy(
            src_ref=gated.at[pl.ds(start, edge)], dst_ref=gated.at[pl.ds(place, edge)],
            send_sem=halo_send.at[up], recv_sem=halo_recv.at[up],
            device_id={"sp": z + 1 if up else z - 1}, device_id_type=MESH,
        )

    @pl.when(z < n - 1)
    def _():
        halo_copy(1).start()

    @pl.when(z > 0)
    def _():
        halo_copy(0).start()

    own_rows = pl.ds(core * chunks, chunks)
    pltpu.make_async_copy(inc.at[own_rows], inc.at[own_rows], point_sem.at[0]).wait()
    mate_copy = pltpu.make_async_remote_copy(
        src_ref=inc.at[own_rows], dst_ref=inc.at[own_rows],
        send_sem=mate_send.at[0], recv_sem=mate_recv.at[0],
        device_id={"tp": mate}, device_id_type=MESH,
    )
    mate_copy.start()

    expert_loads = [
        pltpu.make_async_copy(a, b, w_sem.at[i])
        for i, (a, b) in enumerate(((wg_hbm.at[0], wg), (wu_hbm.at[0], wu), (wd_hbm.at[0], wd)))
    ]
    for load in loads[2:]:
        load.wait()

    tile = rows // 2

    def convolve(s, r):
        start = pl.multiple_of(s * rows + r, 16)
        wide[0] = gated[pl.ds(start, view)].astype(jnp.float32)
        for b in range(1, 8):
            wide[b, pl.ds(0, view - 8)] = wide[0, pl.ds(b, view - 8)]
        value = jnp.zeros((tile, chans), jnp.float32)
        for i in range(taps_count):
            a, b = divmod(edge - half + i, 8)
            value = value + taps_ref[pl.ds(i, 1)] * wide[b, pl.ds(8 * a, tile)]
        mixed[s, pl.ds(pl.multiple_of(r, 16), tile)] = value

    def measure(s):
        value = mixed[s]
        for k, summed in enumerate((value, value * value)):
            line = jnp.broadcast_to(jnp.sum(summed, axis=1, keepdims=True), (rows, rows)).T
            stats[t, s, pl.ds(k, 1)] = line[0:1]
        for p in range(1, tp):
            pltpu.make_async_remote_copy(
                src_ref=stats.at[t, s], dst_ref=stats.at[t, s],
                send_sem=stat_send.at[0], recv_sem=stat_recv.at[s],
                device_id={"tp": lax.rem(t + p, tp)}, device_id_type=MESH,
            ).start()

    def inner(i, carry):
        s = jnp.where(quad == 0, tp - 2 - i, i + 1)
        convolve(s, 0)
        convolve(s, tile)
        measure(s)
        return carry

    def near_edge(i, carry):
        convolve(i * (tp - 1), (1 - i) * tile)
        return carry

    def at_edge(i, carry):
        side = jnp.where(quad == 0, 1 - i, i)
        convolve(side * (tp - 1), side * tile)
        measure(side * (tp - 1))
        return carry

    lax.fori_loop(0, tp - 2, inner, 0)
    lax.fori_loop(0, 2, near_edge, 0)

    ids = ids_ref[...].astype(jnp.float32)
    across = [jnp.broadcast_to(ids[k : k + 1], (rows, rows)) for k in range(top_count)]
    down = [value.T for value in across]
    down_place = lax.broadcasted_iota(jnp.int32, (rows, rows), 0)
    across_place = lax.broadcasted_iota(jnp.int32, (rows, rows), 1)
    tabs[z] = jnp.zeros(tabs.shape[1:], jnp.float32)
    for k in range(top_count):
        count = jnp.zeros((1, rows), jnp.float32)
        for m in range(k + 1):
            same = down[m] == across[k]
            if m == k:
                same = same & (down_place < across_place)
            count = count + jnp.sum(jnp.where(same, 1.0, 0.0), axis=0, keepdims=True)
        tabs[z, pl.ds(k, 1)] = ids[k : k + 1] * cap + count
        tabs[z, pl.ds(top_count + k, 1)] = share_ref[pl.ds(k, 1)]

    @pl.when(z > 0)
    def _():
        halo_copy(1).wait_recv()

    @pl.when(z < n - 1)
    def _():
        halo_copy(0).wait_recv()

    lax.fori_loop(0, 2, at_edge, 0)
    for load in expert_loads:
        load.start()

    def activate_block(s):
        others = stats.at[pl.ds(0, tp - 1), s]
        pltpu.make_async_copy(others, others, stat_recv.at[s]).wait()
        both = stats[0, s]
        for p in range(1, tp):
            both = both + stats[p, s]
        both = both / (chans * tp)
        center = both[0:1]
        scale = lax.rsqrt(both[1:2] - center * center + 0.05)
        center = jnp.broadcast_to(center, (rows, rows)).T[:, 0:1]
        scale = jnp.broadcast_to(scale, (rows, rows)).T[:, 0:1]
        value = (mixed[s] - center) * scale * cgain_ref[...]
        return jax.nn.silu(value).astype(jnp.bfloat16)

    def spot_of(e, which):
        return jnp.where(which == 0, (e + 1) % q_count, e)

    def act_copy(spot):
        return pltpu.make_async_remote_copy(
            src_ref=act_out.at[spot], dst_ref=act_in.at[spot, core],
            send_sem=act_send.at[spot], recv_sem=act_recv.at[spot],
            device_id={"tp": mate}, device_id_type=MESH,
        )

    def product(spot, c):
        left = jnp.concatenate([act_in[spot, 0], act_in[spot, 1]], axis=1)
        right = inc[pl.ds(0, base), c].reshape(base * rows, cols)
        return jnp.dot(left, right, preferred_element_type=jnp.float32)

    def part_copy(spot, k):
        i = lax.rem(spot - quad + q_count, q_count) - 1
        piece = band(k)
        return pltpu.make_async_remote_copy(
            src_ref=psend.at[i, :, piece], dst_ref=inc.at[base + i, :, piece],
            send_sem=part_send.at[i], recv_sem=part_recv.at[i, k],
            device_id={"tp": 2 * spot + core}, device_id_type=MESH,
        )

    for e in range(q_count):
        theirs, ours = spot_of(e, 1 - core), spot_of(e, core)
        act_out[theirs] = activate_block(2 * theirs + 1 - core)
        act_copy(theirs).start()
        act_in[ours, core] = activate_block(2 * ours + core)
        if e == 0:
            mate_copy.wait()
        pltpu.make_async_copy(act_out.at[ours], act_out.at[ours], act_recv.at[ours]).wait()

        @pl.when(ours != quad)
        def _():
            i = lax.rem(ours - quad + q_count, q_count) - 1
            for c in range(PARTS):
                psend[i, c] = product(ours, c).astype(jnp.bfloat16)
            for k in range(len(BANDS) - 1):
                part_copy(ours, k).start()

        @pl.when(ours == quad)
        def _():
            for c in range(PARTS):
                acc[c] = product(ours, c)

    def token_copy(zs, k, side):
        piece = band(k)
        return pltpu.make_async_remote_copy(
            src_ref=toks.at[zs, :, piece], dst_ref=toks.at[zs, :, piece],
            send_sem=tok_send.at[side, zs], recv_sem=tok_recv.at[zs, k],
            device_id={"sp": z + 1 if side else z - 1}, device_id_type=MESH,
        )

    def table_copy(zs, side):
        return pltpu.make_async_remote_copy(
            src_ref=tabs.at[zs], dst_ref=tabs.at[zs],
            send_sem=tab_send.at[side, zs], recv_sem=tab_recv.at[zs],
            device_id={"sp": z + 1 if side else z - 1}, device_id_type=MESH,
        )

    def each_side(zs, act):
        @pl.when((zs <= z) & (z < n - 1))
        def _():
            act(1)

        @pl.when((zs >= z) & (z > 0))
        def _():
            act(0)

    each_side(z, lambda side: table_copy(z, side).start())

    for k in range(len(BANDS) - 1):
        piece = band(k)
        for i in range(1, q_count):
            spot = inc.at[base + i - 1, :, piece]
            pltpu.make_async_copy(spot, spot, part_recv.at[i - 1, k]).wait()
        square = jnp.zeros((piece.size, 1), jnp.float32)
        for c in range(PARTS):
            total = acc[c, piece] + kept[piece, col(c)].astype(jnp.float32)
            for i in range(1, q_count):
                total = total + inc[base + i - 1, c, piece].astype(jnp.float32)
            after = total.astype(jnp.bfloat16)
            kept[piece, col(c)] = after
            after = after.astype(jnp.float32)
            square = square + jnp.sum(after * after, axis=1, keepdims=True)
        norm = lax.rsqrt(square / width + 0.01)
        for c in range(PARTS):
            after = kept[piece, col(c)].astype(jnp.float32)
            toks[z, c, piece] = (after * norm * gain_ref[:, col(c)]).astype(jnp.bfloat16)
        each_side(z, lambda side: token_copy(z, k, side).start())


    upper = z > n - 1 - z
    middle = (z > 0) & (z < n - 1)

    def arrival(j):
        low = jnp.minimum(z, n - 1 - z)
        out = jnp.where(j <= 2 * low, (j + 1) // 2, j - low)
        down = jnp.where(j <= 2 * low, (j % 2 == 1) == upper, upper)
        return jnp.where(down, z - out, z + out)

    def source(i):
        mine = jnp.where(middle, 0, n - 1)
        return jnp.where(i == mine, z, arrival(jnp.where(middle, i, i + 1)))

    def span(g, index):
        return pl.ds(pl.multiple_of(g * group_rows + index * depth, 16), depth)

    def group(g):
        return pl.ds(g * group_rows, group_rows)

    def exchange(j, g, c, from_ref, to_ref, ss, rs):
        page = lax.rem(j, PAGES)
        side = lax.rem(j, 2)
        for p in range(1, tp):
            other = lax.rem(t + p, tp)
            pltpu.make_async_remote_copy(
                src_ref=from_ref.at[side, c, span(g, other)],
                dst_ref=to_ref.at[page, c, span(g, t)],
                send_sem=ss.at[side],
                recv_sem=rs.at[page, g, c],
                device_id={"tp": other},
                device_id_type=MESH,
            ).start()
        to_ref[page, c, span(g, t)] = from_ref[side, c, span(g, t)]

    def wait_pieces(ref, page, g, c, rs):
        part = ref.at[page, c, pl.ds(0, (tp - 1) * depth)]
        pltpu.make_async_copy(part, part, rs.at[page, g, c]).wait()

    def wait_sent(j, from_ref, ss):
        part = from_ref.at[lax.rem(j, 2), :, pl.ds(0, (tp - 1) * cap)]
        pltpu.make_async_copy(part, part, ss.at[lax.rem(j, 2)]).wait()

    def piece_of(h):
        return pl.ds(h * (rows // SPLIT), rows // SPLIT)

    def sum_copy(zs, c, h, side):
        target = z + 1 if side else z - 1
        slot = jnp.where(target == zs, n, zs) if side else zs
        return pltpu.make_async_remote_copy(
            src_ref=toks.at[zs, c, piece_of(h)],
            dst_ref=inc.at[slot, c, piece_of(h)],
            send_sem=sum_send.at[zs],
            recv_sem=sum_recv.at[slot, c, h],
            device_id={"sp": target},
            device_id_type=MESH,
        )

    def names(zs):
        table = tabs[zs]
        start = (z * slots).astype(jnp.float32)
        row = lax.broadcasted_iota(jnp.int32, (slots, rows), 0)
        place = (
            lax.rem(row, group_rows) // depth * cap + row // group_rows * depth + lax.rem(row, depth)
        )
        place = place.astype(jnp.float32) + start
        return place == table[0:1, :], place == table[1:2, :], table

    def passes_on(zs):
        return ((zs < z) & (z < n - 1)) | ((zs > z) & (z > 0))

    def arrive(zs, k):
        spot = toks.at[zs, :, band(k)]
        pltpu.make_async_copy(spot, spot, tok_recv.at[zs, k]).wait()

    def wait_passed(zs, side):
        table_copy(zs, side).wait_send()
        pltpu.make_async_copy(toks.at[zs], toks.at[zs], tok_send.at[side, zs]).wait()

    def hand_on(j):
        zs = arrival(jnp.minimum(j + 1, n - 1))

        @pl.when((j < n - 1) & passes_on(zs))
        def _():
            previous = jnp.where(zs < z, zs + 1, zs - 1)

            @pl.when(previous != z)
            def _():
                each_side(zs, lambda side: wait_passed(previous, side))

            pltpu.make_async_copy(tabs.at[zs], tabs.at[zs], tab_recv.at[zs]).wait()
            each_side(zs, lambda side: table_copy(zs, side).start())
            for k in range(len(BANDS) - 1):
                arrive(zs, k)
                each_side(zs, lambda side: token_copy(zs, k, side).start())

    def take(j):
        zs = source(j)

        @pl.when((zs != z) & jnp.logical_not(passes_on(zs)))
        def _():
            pltpu.make_async_copy(tabs.at[zs], tabs.at[zs], tab_recv.at[zs]).wait()
            for k in range(len(BANDS) - 1):
                arrive(zs, k)

        first, second, _ = names(zs)
        pick = jnp.where(first | second, 1.0, 0.0).astype(jnp.bfloat16)
        side = lax.rem(j, 2)
        for c in range(PARTS):
            comp[side, c] = jnp.dot(
                pick, toks[zs, c], preferred_element_type=jnp.float32
            ).astype(jnp.bfloat16)
            exchange(j, 0, c, comp, arr, piece_send, piece_recv)
        for g in range(1, groups):
            for c in range(PARTS):
                exchange(j, g, c, comp, arr, piece_send, piece_recv)

    def run(j, after_group):
        page = lax.rem(j, PAGES)
        side = lax.rem(j, 2)

        @pl.when(j == 0)
        def _():
            for load in expert_loads:
                load.wait()

        step = 256
        for g in range(groups):
            for c in range(PARTS):
                wait_pieces(arr, page, g, c, piece_recv)
                for f in range(0, hidden_width, step):
                    for to, weights in ((ga, wg), (ua, wu)):
                        value = jnp.dot(
                            arr[page, c, group(g)], weights[col(c), f : f + step],
                            preferred_element_type=jnp.float32,
                        )
                        if c:
                            value = value + to[:, f : f + step]
                        if c < PARTS - 1 or to is ga:
                            to[:, f : f + step] = value
                    if c == PARTS - 1:
                        gate = ga[:, f : f + step]
                        hid[:, f : f + step] = (jax.nn.silu(gate) * value).astype(jnp.bfloat16)
            for c in range(PARTS):
                outs[side, c, group(g)] = jnp.dot(
                    hid[...], wd[:, col(c)], preferred_element_type=jnp.float32
                ).astype(jnp.bfloat16)
                exchange(j, g, c, outs, back, back_send, back_recv)
            after_group(g)
        wait_sent(j, comp, piece_send)

    def merge(j, after_part):
        zs = source(j)
        page = lax.rem(j, PAGES)
        first, second, table = names(zs)
        share = jnp.where(first, table[2:3, :], 0.0) + jnp.where(second, table[3:4, :], 0.0)
        share = share.T
        high = share.astype(jnp.bfloat16)
        rest = (share - high.astype(jnp.float32)).astype(jnp.bfloat16)

        def sent(side):
            @pl.when((zs == (0 if side else n - 1)) & ((zs != z) | jnp.logical_not(middle)))
            def _():
                wait_passed(zs, side)

        each_side(zs, sent)
        for c in range(PARTS):
            for g in range(groups):
                wait_pieces(back, page, g, c, back_recv)
            value = jnp.dot(high, back[page, c], preferred_element_type=jnp.float32) + jnp.dot(
                rest, back[page, c], preferred_element_type=jnp.float32
            )

            @pl.when(zs == z)
            def _():
                acc[c] = value

            @pl.when(zs != z)
            def _():
                toks[zs, c] = value.astype(jnp.bfloat16)

            after_part(zs, c)
        wait_sent(j, outs, back_send)

    def send_sums(zs, c):
        for side in range(2):
            @pl.when((zs > z) & (z == 0) if side else (zs < z) & (z == n - 1))
            def _():
                for h in range(SPLIT):
                    sum_copy(zs, c, h, side).start()

    def relay(turn, p, side):
        zs = turn if side else n - 1 - turn
        c, h = p // SPLIT, p % SPLIT

        @pl.when((z > 0) & (z < turn) if side else (z < n - 1) & (z > n - 1 - turn))
        def _():
            spot = inc.at[zs, c, piece_of(h)]
            pltpu.make_async_copy(spot, spot, sum_recv.at[zs, c, h]).wait()
            toks[zs, c, piece_of(h)] = (
                toks[zs, c, piece_of(h)].astype(jnp.float32)
                + inc[zs, c, piece_of(h)].astype(jnp.float32)
            ).astype(jnp.bfloat16)
            sum_copy(zs, c, h, side).start()

    def relays(turn, start, stop):
        def both(side):
            for p in range(start, stop):
                if p < PARTS * SPLIT:
                    relay(turn, p, side)
                if p >= LAG:
                    relay(turn, p - LAG, 1 - side)

        @pl.when((turn > 0) & upper)
        def _():
            both(0)

        @pl.when((turn > 0) & jnp.logical_not(upper))
        def _():
            both(1)

    def merged(zs, j):
        out = jnp.abs(zs - z)
        low = jnp.minimum(z, n - 1 - z)
        near = jnp.where((zs < z) == upper, 2 * out - 1, 2 * out)
        return jnp.where(out <= low, near, out + low) < j

    def is_early(turn):
        up = (z >= turn) | merged(turn, turn)
        down = (z <= n - 1 - turn) | merged(n - 1 - turn, turn)
        return middle & (turn > 0) & up & down

    pieces = PARTS * SPLIT
    early_stops = (pieces // 4, pieces // 2 + 1, pieces + LAG)

    def early_relays(turn, stop):
        start = (0,) + early_stops
        start = start[start.index(stop) - 1]

        @pl.when(is_early(turn))
        def _():
            relays(turn, start, stop)

    def merge_and_relay(j):
        late = jnp.logical_not(is_early(j))

        def after(zs, c):
            @pl.when(late)
            def _():
                relays(j, c * SPLIT, (c + 1) * SPLIT)

        merge(j, after)

        @pl.when(late)
        def _():
            relays(j, pieces, pieces + LAG)

    def body(j, carry):
        ahead = jnp.where(middle, j + 1, j)

        @pl.when((j == 1) & jnp.logical_not(middle))
        def _():
            merge(j - 1, send_sums)

        @pl.when(ahead < n)
        def _():
            take(ahead)

        @pl.when((j > 1) & jnp.logical_not(middle))
        def _():
            merge(j - 1, send_sums)

        @pl.when(j < n)
        def _():
            early_relays(j - 1, early_stops[0])
            run(j, lambda g: early_relays(j - 1, early_stops[min(g + 1, 1)]) if g == 0 else None)
            early_relays(j - 1, early_stops[2])

        @pl.when(j > 0)
        def _():
            hand_on(j + 1)

        @pl.when((j > 0) & middle)
        def _():
            merge_and_relay(j - 1)

        return carry

    @pl.when(middle)
    def _():
        take(0)
        each_side(z, lambda side: wait_passed(z, side))
        pl.semaphore_signal(turn_sem, inc=1, device_id={"tp": mate}, device_id_type=MESH)
        pl.semaphore_wait(turn_sem, 1)
        hand_on(0)
        hand_on(1)

    lax.fori_loop(0, n + 1, body, 0)

    def final(c, h):
        piece = piece_of(h)

        @pl.when(z < n - 1)
        def _():
            spot = inc.at[z, c, piece]
            pltpu.make_async_copy(spot, spot, sum_recv.at[z, c, h]).wait()
            acc[c, piece] = acc[c, piece] + inc[z, c, piece].astype(jnp.float32)

        @pl.when(z > 0)
        def _():
            spot = inc.at[n, c, piece]
            pltpu.make_async_copy(spot, spot, sum_recv.at[n, c, h]).wait()
            acc[c, piece] = acc[c, piece] + inc[n, c, piece].astype(jnp.float32)

        kept[piece, col(c)] = (
            kept[piece, col(c)].astype(jnp.float32) + acc[c, piece]
        ).astype(jnp.bfloat16)

    for c in range(PARTS):
        for h in range(SPLIT):
            final(c, h)

    def drain(zs, carry):
        @pl.when(zs != z)
        def _():
            pltpu.make_async_copy(toks.at[zs], toks.at[zs], sum_send.at[zs]).wait()

        return carry

    lax.fori_loop(0, n, drain, 0)
    others = stats.at[pl.ds(0, tp - 1)]
    pltpu.make_async_copy(others, others, stat_send.at[0]).wait()
    for e in range(q_count):
        act_copy(e).wait_send()
    for i in range(q_count - 1):
        pltpu.make_async_copy(psend.at[i], psend.at[i], part_send.at[i]).wait()

    @pl.when(z < n - 1)
    def _():
        halo_copy(1).wait_send()

    @pl.when(z > 0)
    def _():
        halo_copy(0).wait_send()


def shards(
    latents,
    conv_value,
    conv_gate,
    conv_taps,
    conv_gain,
    point_weight,
    channel_gain,
    expert_ids,
    expert_weights,
    gate_weight,
    up_weight,
    down_weight,
):
    n, tp = lax.axis_size("sp"), lax.axis_size("tp")
    rows, top_count = expert_ids.shape
    experts = gate_weight.shape[0] * n * tp
    cap = -(-(2 * top_count * rows // experts) // 16) * 16
    block, chans = conv_value.shape
    width = latents.shape[1]
    taps_count = conv_taps.shape[0]
    hidden_width = gate_weight.shape[2]
    slots = tp * cap
    groups = 2 if cap % 32 == 0 else 1
    cols = width // PARTS
    edge = -(-(taps_count // 2) // 16) * 16
    q_count = tp // 2
    spots = max(n + 1, 2 * chans // rows + q_count - 1)
    dma = pltpu.SemaphoreType.DMA
    bf16, f32 = jnp.bfloat16, jnp.float32
    hbm = pl.BlockSpec(memory_space=pltpu.HBM)
    vmem = pltpu.VMEM
    scratch = [
        vmem((block, chans), bf16),
        vmem((block, chans), bf16),
        vmem((taps_count, chans), f32),
        vmem((1, chans), f32),
        vmem((1, width), f32),
        vmem((top_count, rows), jnp.int32),
        vmem((top_count, rows), f32),
        vmem((block + 2 * edge, chans), bf16),
        vmem((8, rows // 2 + 2 * edge, chans), f32),
        vmem((tp, rows, chans), f32),
        vmem((tp, tp, 8, rows), f32),
        vmem((q_count, rows, chans), bf16),
        vmem((q_count, 2, rows, chans), bf16),
        vmem((q_count - 1, PARTS, rows, cols), bf16),
        vmem((n, PARTS, rows, cols), bf16),
        vmem((n, 8, rows), f32),
        vmem((2, PARTS, slots, cols), bf16),
        vmem((2, PARTS, slots, cols), bf16),
        vmem((PAGES, PARTS, slots, cols), bf16),
        vmem((PAGES, PARTS, slots, cols), bf16),
        vmem((spots, PARTS, rows, cols), bf16),
        vmem((PARTS, rows, cols), f32),
        vmem((width, hidden_width), bf16),
        vmem((width, hidden_width), bf16),
        vmem((hidden_width, width), bf16),
        vmem((slots // groups, hidden_width), f32),
        vmem((slots // groups, hidden_width), f32),
        vmem((slots // groups, hidden_width), bf16),
        dma((8,)),
        dma((1,)),
        dma((3,)),
        dma((2,)),
        dma((2,)),
        dma((1,)),
        dma((tp,)),
        dma((1,)),
        dma((1,)),
        dma((q_count,)),
        dma((q_count,)),
        dma((q_count - 1,)),
        dma((q_count - 1, len(BANDS) - 1)),
        dma((2, n)),
        dma((n, len(BANDS) - 1)),
        dma((2, n)),
        dma((n,)),
        dma((2,)),
        dma((PAGES, groups, PARTS)),
        dma((2,)),
        dma((PAGES, groups, PARTS)),
        dma((n,)),
        dma((n + 1, PARTS, SPLIT)),
        pltpu.SemaphoreType.REGULAR,
    ]
    return pl.pallas_call(
        functools.partial(layer_kernel, n, tp, taps_count, cap),
        out_shape=vmem((rows, width), bf16),
        in_specs=[hbm] * 12,
        out_specs=pl.BlockSpec(memory_space=pltpu.VMEM),
        scratch_shapes=scratch,
        compiler_params=pltpu.CompilerParams(
            collective_id=0, has_side_effects=True, vmem_limit_bytes=67043328 - 4 * rows * width
        ),
        name="layer",
    )(
        conv_value, conv_gate, conv_taps, conv_gain[None, :], point_weight, latents,
        channel_gain[None, :], expert_ids.T, expert_weights.T,
        gate_weight, up_weight, down_weight,
    )


def solution(mesh):
    return jax.shard_map(
        shards,
        mesh=mesh,
        in_specs=(
            P(("grp", "sp", "tp"), None),
            P(("grp", "sp"), "tp"),
            P(("grp", "sp"), "tp"),
            P(None, "tp"),
            P("tp"),
            P("tp", None),
            P(),
            P(("grp", "sp", "tp"), None),
            P(("grp", "sp", "tp"), None),
            P(("sp", "tp"), None, None),
            P(("sp", "tp"), None, None),
            P(("sp", "tp"), None, None),
        ),
        out_specs=P(("grp", "sp", "tp"), None),
        check_vma=False,
    )
```

```python
import functools

import jax
import jax.numpy as jnp
from jax import lax
from jax.experimental import pallas as pl
from jax.experimental.pallas import tpu as pltpu
from jax.sharding import PartitionSpec as P


MESH = pl.DeviceIdType.MESH
PARTS = 4
BANDS = (0, 1, 2, 3, 4, 5, 6, 7, 8)
SPLIT = 4
LAG = 5
PAGES = 3


def layer_kernel(
    n, tp, taps_count, cap,
    value_hbm, gate_hbm, taps_hbm, cgain_hbm, weight_hbm, latent_hbm, gain_hbm, ids_hbm, share_hbm,
    wg_hbm, wu_hbm, wd_hbm, kept,
    value_ref, gate_ref, taps_ref, cgain_ref, gain_ref, ids_ref, share_ref,
    gated, wide, mixed, stats, act_out, act_in, psend,
    toks, tabs, comp, outs, arr, back, inc, acc, wg, wu, wd, ga, ua, hid,
    load_sem, point_sem, w_sem, halo_send, halo_recv, stat_send, stat_recv, mate_send, mate_recv,
    act_send, act_recv, part_send, part_recv,
    tok_send, tok_recv, tab_send, tab_recv,
    piece_send, piece_recv, back_send, back_recv, sum_send, sum_recv, turn_sem,
):
    z = lax.axis_index("sp")
    t = lax.axis_index("tp")
    block, chans = value_ref.shape
    rows, width = kept.shape
    slots = tp * cap
    groups = 2 if cap % 32 == 0 else 1
    depth = cap // groups
    group_rows = slots // groups
    hidden_width = wg.shape[1]
    top_count = ids_ref.shape[0]
    cols = width // PARTS
    half = taps_count // 2
    edge = (gated.shape[0] - block) // 2
    view = rows // 2 + 2 * edge
    q_count = tp // 2
    core = lax.rem(t, 2)
    quad = t // 2
    mate = t + 1 - 2 * core
    chunks = chans // rows
    base = 2 * chunks

    def band(k):
        return pl.ds(BANDS[k] * rows // BANDS[-1], (BANDS[k + 1] - BANDS[k]) * rows // BANDS[-1])

    def col(c):
        return pl.ds(c * cols, cols)

    loads = [
        pltpu.make_async_copy(a, b, load_sem.at[i])
        for i, (a, b) in enumerate(
            (
                (value_hbm, value_ref),
                (gate_hbm, gate_ref),
                (taps_hbm, taps_ref),
                (cgain_hbm, cgain_ref),
                (ids_hbm, ids_ref),
                (share_hbm, share_ref),
                (gain_hbm, gain_ref),
                (latent_hbm, kept),
            )
        )
    ]
    for load in loads:
        load.start()

    point_loads = [
        pltpu.make_async_copy(
            weight_hbm.at[pl.ds(b * rows, rows), col(c)],
            inc.at[core * chunks + b, c],
            point_sem.at[0],
        )
        for b in range(chunks)
        for c in range(PARTS)
    ]
    for load in point_loads:
        load.start()

    barrier = pltpu.get_barrier_semaphore()
    for p in range(1, tp):
        pl.semaphore_signal(
            barrier, inc=1, device_id={"tp": lax.rem(t + p, tp)}, device_id_type=MESH
        )

    @pl.when(z > 0)
    def _():
        pl.semaphore_signal(barrier, inc=1, device_id={"sp": z - 1}, device_id_type=MESH)

    @pl.when(z < n - 1)
    def _():
        pl.semaphore_signal(barrier, inc=1, device_id={"sp": z + 1}, device_id_type=MESH)

    @pl.when(z == 0)
    def _():
        gated[pl.ds(0, edge)] = jnp.zeros((edge, chans), jnp.bfloat16)

    @pl.when(z == n - 1)
    def _():
        gated[pl.ds(edge + block, edge)] = jnp.zeros((edge, chans), jnp.bfloat16)

    loads[0].wait()
    loads[1].wait()
    step = 64
    for r in range(0, block, step):
        value = value_ref[pl.ds(r, step)].astype(jnp.float32)
        gate = gate_ref[pl.ds(r, step)].astype(jnp.float32)
        gated[pl.ds(edge + r, step)] = (value * jax.nn.sigmoid(gate)).astype(jnp.bfloat16)

    tile = rows // 2

    def convolve(s, r):
        start = pl.multiple_of(s * rows + r, 16)
        wide[0] = gated[pl.ds(start, view)].astype(jnp.float32)
        for b in range(1, 8):
            wide[b, pl.ds(0, view - 8)] = wide[0, pl.ds(b, view - 8)]
        value = jnp.zeros((tile, chans), jnp.float32)
        for i in range(taps_count):
            a, b = divmod(edge - half + i, 8)
            value = value + taps_ref[pl.ds(i, 1)] * wide[b, pl.ds(8 * a, tile)]
        mixed[s, pl.ds(pl.multiple_of(r, 16), tile)] = value

    opening = jnp.where(quad == 0, 2, 1)
    loads[2].wait()
    convolve(opening, 0)
    convolve(opening, tile)

    peers = tp - 1 + (z > 0).astype(jnp.int32) + (z < n - 1).astype(jnp.int32)
    pl.semaphore_wait(barrier, peers)

    def halo_copy(up):
        start = block if up else edge
        place = 0 if up else edge + block
        return pltpu.make_async_remote_copy(
            src_ref=gated.at[pl.ds(start, edge)], dst_ref=gated.at[pl.ds(place, edge)],
            send_sem=halo_send.at[up], recv_sem=halo_recv.at[up],
            device_id={"sp": z + 1 if up else z - 1}, device_id_type=MESH,
        )

    @pl.when(z < n - 1)
    def _():
        halo_copy(1).start()

    @pl.when(z > 0)
    def _():
        halo_copy(0).start()

    own_rows = pl.ds(core * chunks, chunks)
    pltpu.make_async_copy(inc.at[own_rows], inc.at[own_rows], point_sem.at[0]).wait()
    mate_copy = pltpu.make_async_remote_copy(
        src_ref=inc.at[own_rows], dst_ref=inc.at[own_rows],
        send_sem=mate_send.at[0], recv_sem=mate_recv.at[0],
        device_id={"tp": mate}, device_id_type=MESH,
    )
    mate_copy.start()

    expert_loads = [
        pltpu.make_async_copy(a, b, w_sem.at[i])
        for i, (a, b) in enumerate(((wg_hbm.at[0], wg), (wu_hbm.at[0], wu), (wd_hbm.at[0], wd)))
    ]
    for load in loads[3:]:
        load.wait()

    def measure(s):
        value = mixed[s]
        for k, summed in enumerate((value, value * value)):
            line = jnp.broadcast_to(jnp.sum(summed, axis=1, keepdims=True), (rows, rows)).T
            stats[t, s, pl.ds(k, 1)] = line[0:1]
        for p in range(1, tp):
            pltpu.make_async_remote_copy(
                src_ref=stats.at[t, s], dst_ref=stats.at[t, s],
                send_sem=stat_send.at[0], recv_sem=stat_recv.at[s],
                device_id={"tp": lax.rem(t + p, tp)}, device_id_type=MESH,
            ).start()

    def inner(i, carry):
        s = jnp.where(i == 1, 3 - opening, i + 1)
        convolve(s, 0)
        convolve(s, tile)
        measure(s)
        return carry

    def near_edge(i, carry):
        convolve(i * (tp - 1), (1 - i) * tile)
        return carry

    def at_edge(i, carry):
        side = jnp.where(quad == 0, 1 - i, i)
        convolve(side * (tp - 1), side * tile)
        measure(side * (tp - 1))
        return carry

    measure(opening)
    lax.fori_loop(1, tp - 2, inner, 0)
    lax.fori_loop(0, 2, near_edge, 0)

    ids = ids_ref[...].astype(jnp.float32)
    across = [jnp.broadcast_to(ids[k : k + 1], (rows, rows)) for k in range(top_count)]
    down = [value.T for value in across]
    down_place = lax.broadcasted_iota(jnp.int32, (rows, rows), 0)
    across_place = lax.broadcasted_iota(jnp.int32, (rows, rows), 1)
    tabs[z] = jnp.zeros(tabs.shape[1:], jnp.float32)
    for k in range(top_count):
        count = jnp.zeros((1, rows), jnp.float32)
        for m in range(k + 1):
            same = down[m] == across[k]
            if m == k:
                same = same & (down_place < across_place)
            count = count + jnp.sum(jnp.where(same, 1.0, 0.0), axis=0, keepdims=True)
        tabs[z, pl.ds(k, 1)] = ids[k : k + 1] * cap + count
        tabs[z, pl.ds(top_count + k, 1)] = share_ref[pl.ds(k, 1)]

    def activate_block(s):
        others = stats.at[pl.ds(0, tp - 1), s]
        pltpu.make_async_copy(others, others, stat_recv.at[s]).wait()
        both = stats[0, s]
        for p in range(1, tp):
            both = both + stats[p, s]
        both = both / (chans * tp)
        center = both[0:1]
        scale = lax.rsqrt(both[1:2] - center * center + 0.05)
        center = jnp.broadcast_to(center, (rows, rows)).T[:, 0:1]
        scale = jnp.broadcast_to(scale, (rows, rows)).T[:, 0:1]
        value = (mixed[s] - center) * scale * cgain_ref[...]
        return jax.nn.silu(value).astype(jnp.bfloat16)

    def spot_of(e, which):
        return jnp.where(which == 0, (e + 1) % q_count, e)

    def act_copy(spot):
        return pltpu.make_async_remote_copy(
            src_ref=act_out.at[spot], dst_ref=act_in.at[spot, core],
            send_sem=act_send.at[spot], recv_sem=act_recv.at[spot],
            device_id={"tp": mate}, device_id_type=MESH,
        )

    def share_block(s):
        @pl.when(lax.rem(s, 2) == core)
        def _():
            act_in[s // 2, core] = activate_block(s)

        @pl.when(lax.rem(s, 2) != core)
        def _():
            act_out[s // 2] = activate_block(s)
            act_copy(s // 2).start()

    share_block(opening)

    @pl.when(z > 0)
    def _():
        halo_copy(1).wait_recv()

    @pl.when(z < n - 1)
    def _():
        halo_copy(0).wait_recv()

    lax.fori_loop(0, 2, at_edge, 0)
    for load in expert_loads:
        load.start()

    def product(spot, c):
        left = jnp.concatenate([act_in[spot, 0], act_in[spot, 1]], axis=1)
        right = inc[pl.ds(0, base), c].reshape(base * rows, cols)
        return jnp.dot(left, right, preferred_element_type=jnp.float32)

    def part_copy(spot, k):
        i = lax.rem(spot - quad + q_count, q_count) - 1
        piece = band(k)
        return pltpu.make_async_remote_copy(
            src_ref=psend.at[i, :, piece], dst_ref=inc.at[base + i, :, piece],
            send_sem=part_send.at[i], recv_sem=part_recv.at[i, k],
            device_id={"tp": 2 * spot + core}, device_id_type=MESH,
        )

    def token_copy(zs, k, side):
        piece = band(k)
        return pltpu.make_async_remote_copy(
            src_ref=toks.at[zs, :, piece], dst_ref=toks.at[zs, :, piece],
            send_sem=tok_send.at[side, zs], recv_sem=tok_recv.at[zs, k // 2],
            device_id={"sp": z + 1 if side else z - 1}, device_id_type=MESH,
        )

    def table_copy(zs, side):
        return pltpu.make_async_remote_copy(
            src_ref=tabs.at[zs], dst_ref=tabs.at[zs],
            send_sem=tab_send.at[side, zs], recv_sem=tab_recv.at[zs],
            device_id={"sp": z + 1 if side else z - 1}, device_id_type=MESH,
        )

    def each_side(zs, act):
        @pl.when((zs <= z) & (z < n - 1))
        def _():
            act(1)

        @pl.when((zs >= z) & (z > 0))
        def _():
            act(0)

    def send_band(k):
        piece = band(k)
        for i in range(1, q_count):
            spot = inc.at[base + i - 1, :, piece]
            pltpu.make_async_copy(spot, spot, part_recv.at[i - 1, k]).wait()
        square = jnp.zeros((piece.size, 1), jnp.float32)
        for c in range(PARTS):
            total = acc[c, piece] + kept[piece, col(c)].astype(jnp.float32)
            for i in range(1, q_count):
                total = total + inc[base + i - 1, c, piece].astype(jnp.float32)
            after = total.astype(jnp.bfloat16)
            kept[piece, col(c)] = after
            after = after.astype(jnp.float32)
            square = square + jnp.sum(after * after, axis=1, keepdims=True)
        norm = lax.rsqrt(square / width + 0.01)
        for c in range(PARTS):
            after = kept[piece, col(c)].astype(jnp.float32)
            toks[z, c, piece] = (after * norm * gain_ref[:, col(c)]).astype(jnp.bfloat16)
        each_side(z, lambda side: token_copy(z, k, side).start())

    for e in range(q_count):
        theirs, ours = spot_of(e, 1 - core), spot_of(e, core)
        if e == 0:
            share_block(3 - opening)
            mate_copy.wait()
        else:
            act_out[theirs] = activate_block(2 * theirs + 1 - core)
            act_copy(theirs).start()
            act_in[ours, core] = activate_block(2 * ours + core)
        pltpu.make_async_copy(act_out.at[ours], act_out.at[ours], act_recv.at[ours]).wait()

        @pl.when(ours != quad)
        def _():
            i = lax.rem(ours - quad + q_count, q_count) - 1
            for c in range(PARTS):
                psend[i, c] = product(ours, c).astype(jnp.bfloat16)
            for k in range(len(BANDS) - 1):
                part_copy(ours, k).start()

        @pl.when(ours == quad)
        def _():
            for c in range(PARTS):
                acc[c] = product(ours, c)

    each_side(z, lambda side: table_copy(z, side).start())
    for k in range(len(BANDS) - 1):
        send_band(k)


    upper = z > n - 1 - z
    middle = (z > 0) & (z < n - 1)

    def arrival(j):
        low = jnp.minimum(z, n - 1 - z)
        out = jnp.where(j <= 2 * low, (j + 1) // 2, j - low)
        down = jnp.where(j <= 2 * low, (j % 2 == 1) == upper, upper)
        return jnp.where(down, z - out, z + out)

    def source(i):
        mine = jnp.where(middle, 0, n - 1)
        return jnp.where(i == mine, z, arrival(jnp.where(middle, i, i + 1)))

    def span(g, index):
        return pl.ds(pl.multiple_of(g * group_rows + index * depth, 16), depth)

    def group(g):
        return pl.ds(g * group_rows, group_rows)

    def exchange(j, g, c, from_ref, to_ref, ss, rs):
        page = lax.rem(j, PAGES)
        side = lax.rem(j, 2)
        for p in range(1, tp):
            other = lax.rem(t + p, tp)
            pltpu.make_async_remote_copy(
                src_ref=from_ref.at[side, c, span(g, other)],
                dst_ref=to_ref.at[page, c, span(g, t)],
                send_sem=ss.at[side],
                recv_sem=rs.at[page, g, c] if to_ref is arr else rs.at[page, c],
                device_id={"tp": other},
                device_id_type=MESH,
            ).start()
        to_ref[page, c, span(g, t)] = from_ref[side, c, span(g, t)]

    def wait_pieces(ref, page, g, c, rs):
        part = ref.at[page, c, pl.ds(0, (tp - 1) * depth)]
        pltpu.make_async_copy(part, part, rs.at[page, g, c]).wait()

    def wait_sent(j, from_ref, ss):
        part = from_ref.at[lax.rem(j, 2), :, pl.ds(0, (tp - 1) * cap)]
        pltpu.make_async_copy(part, part, ss.at[lax.rem(j, 2)]).wait()

    def piece_of(h):
        return pl.ds(h * (rows // SPLIT), rows // SPLIT)

    def sum_copy(zs, c, h, side):
        target = z + 1 if side else z - 1
        slot = jnp.where(target == zs, n, zs) if side else zs
        return pltpu.make_async_remote_copy(
            src_ref=toks.at[zs, c, piece_of(h)],
            dst_ref=inc.at[slot, c, piece_of(h)],
            send_sem=sum_send.at[zs],
            recv_sem=sum_recv.at[slot, c, h],
            device_id={"sp": target},
            device_id_type=MESH,
        )

    def names(zs):
        table = tabs[zs]
        start = (z * slots).astype(jnp.float32)
        row = lax.broadcasted_iota(jnp.int32, (slots, rows), 0)
        place = (
            lax.rem(row, group_rows) // depth * cap + row // group_rows * depth + lax.rem(row, depth)
        )
        place = place.astype(jnp.float32) + start
        return place == table[0:1, :], place == table[1:2, :], table

    def passes_on(zs):
        return ((zs < z) & (z < n - 1)) | ((zs > z) & (z > 0))

    def arrive(zs, k):
        spot = toks.at[zs, :, pl.ds(band(k).start, band(k).size + band(k + 1).size)]
        pltpu.make_async_copy(spot, spot, tok_recv.at[zs, k // 2]).wait()

    def wait_passed(zs, side):
        table_copy(zs, side).wait_send()
        pltpu.make_async_copy(toks.at[zs], toks.at[zs], tok_send.at[side, zs]).wait()

    def hand_on(j):
        zs = arrival(jnp.minimum(j + 1, n - 1))

        @pl.when((j < n - 1) & passes_on(zs))
        def _():
            previous = jnp.where(zs < z, zs + 1, zs - 1)

            @pl.when(previous != z)
            def _():
                each_side(zs, lambda side: wait_passed(previous, side))

            pltpu.make_async_copy(tabs.at[zs], tabs.at[zs], tab_recv.at[zs]).wait()
            each_side(zs, lambda side: table_copy(zs, side).start())
            for k in range(len(BANDS) - 1):
                if k % 2 == 0:
                    arrive(zs, k)
                each_side(zs, lambda side: token_copy(zs, k, side).start())

    def take(j):
        zs = source(j)

        @pl.when((zs != z) & jnp.logical_not(passes_on(zs)))
        def _():
            pltpu.make_async_copy(tabs.at[zs], tabs.at[zs], tab_recv.at[zs]).wait()
            for k in range(0, len(BANDS) - 1, 2):
                arrive(zs, k)

        first, second, _ = names(zs)
        pick = jnp.where(first | second, 1.0, 0.0).astype(jnp.bfloat16)
        side = lax.rem(j, 2)
        for c in range(PARTS):
            comp[side, c] = jnp.dot(
                pick, toks[zs, c], preferred_element_type=jnp.float32
            ).astype(jnp.bfloat16)
            exchange(j, 0, c, comp, arr, piece_send, piece_recv)
        for g in range(1, groups):
            for c in range(PARTS):
                exchange(j, g, c, comp, arr, piece_send, piece_recv)

    def run(j, after_group):
        page = lax.rem(j, PAGES)
        side = lax.rem(j, 2)

        @pl.when(j == 0)
        def _():
            for load in expert_loads:
                load.wait()

        step = 256
        for g in range(groups):
            for c in range(PARTS):
                wait_pieces(arr, page, g, c, piece_recv)
                for f in range(0, hidden_width, step):
                    for to, weights in ((ga, wg), (ua, wu)):
                        value = jnp.dot(
                            arr[page, c, group(g)], weights[col(c), f : f + step],
                            preferred_element_type=jnp.float32,
                        )
                        if c:
                            value = value + to[:, f : f + step]
                        if c < PARTS - 1 or to is ga:
                            to[:, f : f + step] = value
                    if c == PARTS - 1:
                        gate = ga[:, f : f + step]
                        hid[:, f : f + step] = (jax.nn.silu(gate) * value).astype(jnp.bfloat16)
            for c in range(PARTS):
                outs[side, c, group(g)] = jnp.dot(
                    hid[...], wd[:, col(c)], preferred_element_type=jnp.float32
                ).astype(jnp.bfloat16)
                exchange(j, g, c, outs, back, back_send, back_recv)
            after_group(g)
        wait_sent(j, comp, piece_send)

    def merge(j, after_part):
        zs = source(j)
        page = lax.rem(j, PAGES)
        first, second, table = names(zs)
        share = jnp.where(first, table[2:3, :], 0.0) + jnp.where(second, table[3:4, :], 0.0)
        share = share.T
        high = share.astype(jnp.bfloat16)
        rest = (share - high.astype(jnp.float32)).astype(jnp.bfloat16)

        def sent(side):
            @pl.when((zs == (0 if side else n - 1)) & ((zs != z) | jnp.logical_not(middle)))
            def _():
                wait_passed(zs, side)

        each_side(zs, sent)
        for c in range(PARTS):
            part = back.at[page, c, pl.ds(0, (tp - 1) * cap)]
            pltpu.make_async_copy(part, part, back_recv.at[page, c]).wait()
            value = jnp.dot(high, back[page, c], preferred_element_type=jnp.float32) + jnp.dot(
                rest, back[page, c], preferred_element_type=jnp.float32
            )

            @pl.when(zs == z)
            def _():
                acc[c] = value

            @pl.when(zs != z)
            def _():
                toks[zs, c] = value.astype(jnp.bfloat16)

            after_part(zs, c)
        wait_sent(j, outs, back_send)

    def send_sums(zs, c):
        for side in range(2):
            @pl.when((zs > z) & (z == 0) if side else (zs < z) & (z == n - 1))
            def _():
                for h in range(SPLIT):
                    sum_copy(zs, c, h, side).start()

    def relay(turn, p, side):
        zs = turn if side else n - 1 - turn
        c, h = p // SPLIT, p % SPLIT

        @pl.when((z > 0) & (z < turn) if side else (z < n - 1) & (z > n - 1 - turn))
        def _():
            spot = inc.at[zs, c, piece_of(h)]
            pltpu.make_async_copy(spot, spot, sum_recv.at[zs, c, h]).wait()
            toks[zs, c, piece_of(h)] = (
                toks[zs, c, piece_of(h)].astype(jnp.float32)
                + inc[zs, c, piece_of(h)].astype(jnp.float32)
            ).astype(jnp.bfloat16)
            sum_copy(zs, c, h, side).start()

    def relays(turn, start, stop):
        def both(side):
            for p in range(start, stop):
                if p < PARTS * SPLIT:
                    relay(turn, p, side)
                if p >= LAG:
                    relay(turn, p - LAG, 1 - side)

        @pl.when((turn > 0) & upper)
        def _():
            both(0)

        @pl.when((turn > 0) & jnp.logical_not(upper))
        def _():
            both(1)

    def merged(zs, j):
        out = jnp.abs(zs - z)
        low = jnp.minimum(z, n - 1 - z)
        near = jnp.where((zs < z) == upper, 2 * out - 1, 2 * out)
        return jnp.where(out <= low, near, out + low) < j

    def is_early(turn):
        up = (z >= turn) | merged(turn, turn)
        down = (z <= n - 1 - turn) | merged(n - 1 - turn, turn)
        return middle & (turn > 0) & up & down

    pieces = PARTS * SPLIT
    early_stops = (pieces // 4, pieces // 2 + 1, pieces + LAG)

    def early_relays(turn, stop):
        start = (0,) + early_stops
        start = start[start.index(stop) - 1]

        @pl.when(is_early(turn))
        def _():
            relays(turn, start, stop)

    def merge_and_relay(j):
        late = jnp.logical_not(is_early(j))

        def after(zs, c):
            @pl.when(late)
            def _():
                relays(j, c * SPLIT, (c + 1) * SPLIT)

        merge(j, after)

        @pl.when(late)
        def _():
            relays(j, pieces, pieces + LAG)

    def body(j, carry):
        ahead = jnp.where(middle, j + 1, j)

        @pl.when((j == 1) & jnp.logical_not(middle))
        def _():
            merge(j - 1, send_sums)

        @pl.when(ahead < n)
        def _():
            take(ahead)

        @pl.when((j > 1) & jnp.logical_not(middle))
        def _():
            merge(j - 1, send_sums)

        @pl.when(j < n)
        def _():
            early_relays(j - 1, early_stops[0])
            run(j, lambda g: early_relays(j - 1, early_stops[min(g + 1, 1)]) if g == 0 else None)
            early_relays(j - 1, early_stops[2])

        @pl.when(j > 0)
        def _():
            hand_on(j + 1)

        @pl.when((j > 0) & middle)
        def _():
            merge_and_relay(j - 1)

        return carry

    @pl.when(middle)
    def _():
        take(0)
        each_side(z, lambda side: wait_passed(z, side))
        pl.semaphore_signal(turn_sem, inc=1, device_id={"tp": mate}, device_id_type=MESH)
        pl.semaphore_wait(turn_sem, 1)
        hand_on(0)
        hand_on(1)

    lax.fori_loop(0, n + 1, body, 0)

    def final(c, h):
        piece = piece_of(h)

        @pl.when(z < n - 1)
        def _():
            spot = inc.at[z, c, piece]
            pltpu.make_async_copy(spot, spot, sum_recv.at[z, c, h]).wait()
            acc[c, piece] = acc[c, piece] + inc[z, c, piece].astype(jnp.float32)

        @pl.when(z > 0)
        def _():
            spot = inc.at[n, c, piece]
            pltpu.make_async_copy(spot, spot, sum_recv.at[n, c, h]).wait()
            acc[c, piece] = acc[c, piece] + inc[n, c, piece].astype(jnp.float32)

        kept[piece, col(c)] = (
            kept[piece, col(c)].astype(jnp.float32) + acc[c, piece]
        ).astype(jnp.bfloat16)

    for c in range(PARTS):
        for h in range(SPLIT):
            final(c, h)

    def drain(zs, carry):
        @pl.when(zs != z)
        def _():
            pltpu.make_async_copy(toks.at[zs], toks.at[zs], sum_send.at[zs]).wait()

        return carry

    lax.fori_loop(0, n, drain, 0)
    others = stats.at[pl.ds(0, tp - 1)]
    pltpu.make_async_copy(others, others, stat_send.at[0]).wait()
    for e in range(q_count):
        act_copy(e).wait_send()
    for i in range(q_count - 1):
        pltpu.make_async_copy(psend.at[i], psend.at[i], part_send.at[i]).wait()

    @pl.when(z < n - 1)
    def _():
        halo_copy(1).wait_send()

    @pl.when(z > 0)
    def _():
        halo_copy(0).wait_send()


def shards(
    latents,
    conv_value,
    conv_gate,
    conv_taps,
    conv_gain,
    point_weight,
    channel_gain,
    expert_ids,
    expert_weights,
    gate_weight,
    up_weight,
    down_weight,
):
    n, tp = lax.axis_size("sp"), lax.axis_size("tp")
    rows, top_count = expert_ids.shape
    experts = gate_weight.shape[0] * n * tp
    cap = -(-(2 * top_count * rows // experts) // 16) * 16
    block, chans = conv_value.shape
    width = latents.shape[1]
    taps_count = conv_taps.shape[0]
    hidden_width = gate_weight.shape[2]
    slots = tp * cap
    groups = 2 if cap % 32 == 0 else 1
    cols = width // PARTS
    edge = -(-(taps_count // 2) // 16) * 16
    q_count = tp // 2
    spots = max(n + 1, 2 * chans // rows + q_count - 1)
    dma = pltpu.SemaphoreType.DMA
    bf16, f32 = jnp.bfloat16, jnp.float32
    hbm = pl.BlockSpec(memory_space=pltpu.HBM)
    vmem = pltpu.VMEM
    scratch = [
        vmem((block, chans), bf16),
        vmem((block, chans), bf16),
        vmem((taps_count, chans), f32),
        vmem((1, chans), f32),
        vmem((1, width), f32),
        vmem((top_count, rows), jnp.int32),
        vmem((top_count, rows), f32),
        vmem((block + 2 * edge, chans), bf16),
        vmem((8, rows // 2 + 2 * edge, chans), f32),
        vmem((tp, rows, chans), f32),
        vmem((tp, tp, 8, rows), f32),
        vmem((q_count, rows, chans), bf16),
        vmem((q_count, 2, rows, chans), bf16),
        vmem((q_count - 1, PARTS, rows, cols), bf16),
        vmem((n, PARTS, rows, cols), bf16),
        vmem((n, 8, rows), f32),
        vmem((2, PARTS, slots, cols), bf16),
        vmem((2, PARTS, slots, cols), bf16),
        vmem((PAGES, PARTS, slots, cols), bf16),
        vmem((PAGES, PARTS, slots, cols), bf16),
        vmem((spots, PARTS, rows, cols), bf16),
        vmem((PARTS, rows, cols), f32),
        vmem((width, hidden_width), bf16),
        vmem((width, hidden_width), bf16),
        vmem((hidden_width, width), bf16),
        vmem((slots // groups, hidden_width), f32),
        vmem((slots // groups, hidden_width), f32),
        vmem((slots // groups, hidden_width), bf16),
        dma((8,)),
        dma((1,)),
        dma((3,)),
        dma((2,)),
        dma((2,)),
        dma((1,)),
        dma((tp,)),
        dma((1,)),
        dma((1,)),
        dma((q_count,)),
        dma((q_count,)),
        dma((q_count - 1,)),
        dma((q_count - 1, len(BANDS) - 1)),
        dma((2, n)),
        dma((n, (len(BANDS) - 1) // 2)),
        dma((2, n)),
        dma((n,)),
        dma((2,)),
        dma((PAGES, groups, PARTS)),
        dma((2,)),
        dma((PAGES, PARTS)),
        dma((n,)),
        dma((n + 1, PARTS, SPLIT)),
        pltpu.SemaphoreType.REGULAR,
    ]
    return pl.pallas_call(
        functools.partial(layer_kernel, n, tp, taps_count, cap),
        out_shape=vmem((rows, width), bf16),
        in_specs=[hbm] * 12,
        out_specs=pl.BlockSpec(memory_space=pltpu.VMEM),
        scratch_shapes=scratch,
        compiler_params=pltpu.CompilerParams(
            collective_id=0, has_side_effects=True, vmem_limit_bytes=67043328 - 4 * rows * width
        ),
        name="layer",
    )(
        conv_value, conv_gate, conv_taps, conv_gain[None, :], point_weight, latents,
        channel_gain[None, :], expert_ids.T, expert_weights.T,
        gate_weight, up_weight, down_weight,
    )


def solution(mesh):
    return jax.shard_map(
        shards,
        mesh=mesh,
        in_specs=(
            P(("grp", "sp", "tp"), None),
            P(("grp", "sp"), "tp"),
            P(("grp", "sp"), "tp"),
            P(None, "tp"),
            P("tp"),
            P("tp", None),
            P(),
            P(("grp", "sp", "tp"), None),
            P(("grp", "sp", "tp"), None),
            P(("sp", "tp"), None, None),
            P(("sp", "tp"), None, None),
            P(("sp", "tp"), None, None),
        ),
        out_specs=P(("grp", "sp", "tp"), None),
        check_vma=False,
    )
```

```python
import functools

import jax
import jax.numpy as jnp
from jax import lax
from jax.experimental import pallas as pl
from jax.experimental.pallas import tpu as pltpu
from jax.sharding import PartitionSpec as P


MESH = pl.DeviceIdType.MESH
PARTS = 4
BANDS = (0, 1, 2, 3, 4, 5, 6, 7, 8)
SPLIT = 4
LAG = 5
PAGES = 3


def layer_kernel(
    n, tp, taps_count, cap,
    value_hbm, gate_hbm, taps_hbm, cgain_hbm, weight_hbm, latent_hbm, gain_hbm, ids_hbm, share_hbm,
    wg_hbm, wu_hbm, wd_hbm, kept,
    value_ref, gate_ref, taps_ref, cgain_ref, gain_ref, ids_ref, share_ref,
    gated, wide, mixed, stats, act_out, act_in, psend,
    toks, tabs, comp, outs, arr, back, inc, acc, wg, wu, wd, ga, ua, hid,
    load_sem, point_sem, w_sem, halo_send, halo_recv, stat_send, stat_recv, mate_send, mate_recv,
    act_send, act_recv, part_send, part_recv,
    tok_send, tok_recv, tab_send, tab_recv,
    piece_send, piece_recv, back_send, back_recv, sum_send, sum_recv, turn_sem,
):
    z = lax.axis_index("sp")
    t = lax.axis_index("tp")
    block, chans = value_ref.shape
    rows, width = kept.shape
    slots = tp * cap
    groups = 2 if cap % 32 == 0 else 1
    depth = cap // groups
    group_rows = slots // groups
    hidden_width = wg.shape[1]
    top_count = ids_ref.shape[0]
    cols = width // PARTS
    half = taps_count // 2
    edge = (gated.shape[0] - block) // 2
    view = rows // 2 + 2 * edge
    q_count = tp // 2
    core = lax.rem(t, 2)
    quad = t // 2
    mate = t + 1 - 2 * core
    chunks = chans // rows
    base = 2 * chunks

    def band(k):
        return pl.ds(BANDS[k] * rows // BANDS[-1], (BANDS[k + 1] - BANDS[k]) * rows // BANDS[-1])

    def col(c):
        return pl.ds(c * cols, cols)

    loads = [
        pltpu.make_async_copy(a, b, load_sem.at[i])
        for i, (a, b) in enumerate(
            (
                (value_hbm, value_ref),
                (gate_hbm, gate_ref),
                (taps_hbm, taps_ref),
                (cgain_hbm, cgain_ref),
                (ids_hbm, ids_ref),
                (share_hbm, share_ref),
                (gain_hbm, gain_ref),
                (latent_hbm, kept),
            )
        )
    ]
    for load in loads:
        load.start()

    point_loads = [
        pltpu.make_async_copy(
            weight_hbm.at[pl.ds(b * rows, rows), col(c)],
            inc.at[core * chunks + b, c],
            point_sem.at[0],
        )
        for b in range(chunks)
        for c in range(PARTS)
    ]
    for load in point_loads:
        load.start()

    barrier = pltpu.get_barrier_semaphore()
    for p in range(1, tp):
        pl.semaphore_signal(
            barrier, inc=1, device_id={"tp": lax.rem(t + p, tp)}, device_id_type=MESH
        )

    @pl.when(z > 0)
    def _():
        pl.semaphore_signal(barrier, inc=1, device_id={"sp": z - 1}, device_id_type=MESH)

    @pl.when(z < n - 1)
    def _():
        pl.semaphore_signal(barrier, inc=1, device_id={"sp": z + 1}, device_id_type=MESH)

    @pl.when(z == 0)
    def _():
        gated[pl.ds(0, edge)] = jnp.zeros((edge, chans), jnp.bfloat16)

    @pl.when(z == n - 1)
    def _():
        gated[pl.ds(edge + block, edge)] = jnp.zeros((edge, chans), jnp.bfloat16)

    loads[0].wait()
    loads[1].wait()
    step = 64
    for r in range(0, block, step):
        value = value_ref[pl.ds(r, step)].astype(jnp.float32)
        gate = gate_ref[pl.ds(r, step)].astype(jnp.float32)
        gated[pl.ds(edge + r, step)] = (value * jax.nn.sigmoid(gate)).astype(jnp.bfloat16)

    tile = rows // 2

    def convolve(s, r):
        start = pl.multiple_of(s * rows + r, 16)
        wide[0] = gated[pl.ds(start, view)].astype(jnp.float32)
        for b in range(1, 8):
            wide[b, pl.ds(0, view - 8)] = wide[0, pl.ds(b, view - 8)]
        value = jnp.zeros((tile, chans), jnp.float32)
        for i in range(taps_count):
            a, b = divmod(edge - half + i, 8)
            value = value + taps_ref[pl.ds(i, 1)] * wide[b, pl.ds(8 * a, tile)]
        mixed[s, pl.ds(pl.multiple_of(r, 16), tile)] = value

    opening = jnp.where(quad == 0, 2, 1)
    loads[2].wait()
    convolve(opening, 0)
    convolve(opening, tile)

    peers = tp - 1 + (z > 0).astype(jnp.int32) + (z < n - 1).astype(jnp.int32)
    pl.semaphore_wait(barrier, peers)

    def halo_copy(up):
        start = block if up else edge
        place = 0 if up else edge + block
        return pltpu.make_async_remote_copy(
            src_ref=gated.at[pl.ds(start, edge)], dst_ref=gated.at[pl.ds(place, edge)],
            send_sem=halo_send.at[up], recv_sem=halo_recv.at[up],
            device_id={"sp": z + 1 if up else z - 1}, device_id_type=MESH,
        )

    @pl.when(z < n - 1)
    def _():
        halo_copy(1).start()

    @pl.when(z > 0)
    def _():
        halo_copy(0).start()

    own_rows = pl.ds(core * chunks, chunks)
    pltpu.make_async_copy(inc.at[own_rows], inc.at[own_rows], point_sem.at[0]).wait()
    mate_copy = pltpu.make_async_remote_copy(
        src_ref=inc.at[own_rows], dst_ref=inc.at[own_rows],
        send_sem=mate_send.at[0], recv_sem=mate_recv.at[0],
        device_id={"tp": mate}, device_id_type=MESH,
    )
    mate_copy.start()

    expert_loads = [
        pltpu.make_async_copy(a, b, w_sem.at[i])
        for i, (a, b) in enumerate(((wg_hbm.at[0], wg), (wu_hbm.at[0], wu), (wd_hbm.at[0], wd)))
    ]
    for load in loads[3:]:
        load.wait()

    def measure(s):
        value = mixed[s]
        for k, summed in enumerate((value, value * value)):
            line = jnp.broadcast_to(jnp.sum(summed, axis=1, keepdims=True), (rows, rows)).T
            stats[t, s, pl.ds(k, 1)] = line[0:1]
        for p in range(1, tp):
            pltpu.make_async_remote_copy(
                src_ref=stats.at[t, s], dst_ref=stats.at[t, s],
                send_sem=stat_send.at[0], recv_sem=stat_recv.at[s],
                device_id={"tp": lax.rem(t + p, tp)}, device_id_type=MESH,
            ).start()

    def inner(i, carry):
        s = jnp.where(i == 1, 3 - opening, i + 1)
        convolve(s, 0)
        convolve(s, tile)
        measure(s)
        return carry

    def near_edge(i, carry):
        convolve(i * (tp - 1), (1 - i) * tile)
        return carry

    def at_edge(i, carry):
        side = jnp.where(quad == 0, 1 - i, i)
        convolve(side * (tp - 1), side * tile)
        measure(side * (tp - 1))
        return carry

    measure(opening)
    lax.fori_loop(1, tp - 2, inner, 0)
    lax.fori_loop(0, 2, near_edge, 0)

    ids = ids_ref[...].astype(jnp.float32)
    across = [jnp.broadcast_to(ids[k : k + 1], (rows, rows)) for k in range(top_count)]
    down = [value.T for value in across]
    down_place = lax.broadcasted_iota(jnp.int32, (rows, rows), 0)
    across_place = lax.broadcasted_iota(jnp.int32, (rows, rows), 1)
    tabs[z] = jnp.zeros(tabs.shape[1:], jnp.float32)
    for k in range(top_count):
        count = jnp.zeros((1, rows), jnp.float32)
        for m in range(k + 1):
            same = down[m] == across[k]
            if m == k:
                same = same & (down_place < across_place)
            count = count + jnp.sum(jnp.where(same, 1.0, 0.0), axis=0, keepdims=True)
        tabs[z, pl.ds(k, 1)] = ids[k : k + 1] * cap + count
        tabs[z, pl.ds(top_count + k, 1)] = share_ref[pl.ds(k, 1)]

    def activate_block(s):
        others = stats.at[pl.ds(0, tp - 1), s]
        pltpu.make_async_copy(others, others, stat_recv.at[s]).wait()
        both = stats[0, s]
        for p in range(1, tp):
            both = both + stats[p, s]
        both = both / (chans * tp)
        center = both[0:1]
        scale = lax.rsqrt(both[1:2] - center * center + 0.05)
        center = jnp.broadcast_to(center, (rows, rows)).T[:, 0:1]
        scale = jnp.broadcast_to(scale, (rows, rows)).T[:, 0:1]
        value = (mixed[s] - center) * scale * cgain_ref[...]
        return jax.nn.silu(value).astype(jnp.bfloat16)

    def spot_of(e, which):
        return jnp.where(which == 0, (e + 1) % q_count, e)

    def act_copy(spot):
        return pltpu.make_async_remote_copy(
            src_ref=act_out.at[spot], dst_ref=act_in.at[spot, core],
            send_sem=act_send.at[spot], recv_sem=act_recv.at[spot],
            device_id={"tp": mate}, device_id_type=MESH,
        )

    def share_block(s):
        @pl.when(lax.rem(s, 2) == core)
        def _():
            act_in[s // 2, core] = activate_block(s)

        @pl.when(lax.rem(s, 2) != core)
        def _():
            act_out[s // 2] = activate_block(s)
            act_copy(s // 2).start()

    share_block(opening)

    @pl.when(z > 0)
    def _():
        halo_copy(1).wait_recv()

    @pl.when(z < n - 1)
    def _():
        halo_copy(0).wait_recv()

    lax.fori_loop(0, 2, at_edge, 0)
    for load in expert_loads:
        load.start()

    def product(spot, c):
        left = jnp.concatenate([act_in[spot, 0], act_in[spot, 1]], axis=1)
        right = inc[pl.ds(0, base), c].reshape(base * rows, cols)
        return jnp.dot(left, right, preferred_element_type=jnp.float32)

    def part_copy(spot, k):
        i = lax.rem(spot - quad + q_count, q_count) - 1
        piece = band(k)
        return pltpu.make_async_remote_copy(
            src_ref=psend.at[i, :, piece], dst_ref=inc.at[base + i, :, piece],
            send_sem=part_send.at[i], recv_sem=part_recv.at[i, k],
            device_id={"tp": 2 * spot + core}, device_id_type=MESH,
        )

    def token_copy(zs, k, side):
        piece = band(k)
        return pltpu.make_async_remote_copy(
            src_ref=toks.at[zs, :, piece], dst_ref=toks.at[zs, :, piece],
            send_sem=tok_send.at[side, zs], recv_sem=tok_recv.at[zs, k // 2],
            device_id={"sp": z + 1 if side else z - 1}, device_id_type=MESH,
        )

    def table_copy(zs, side):
        return pltpu.make_async_remote_copy(
            src_ref=tabs.at[zs], dst_ref=tabs.at[zs],
            send_sem=tab_send.at[side, zs], recv_sem=tab_recv.at[zs],
            device_id={"sp": z + 1 if side else z - 1}, device_id_type=MESH,
        )

    def each_side(zs, act):
        @pl.when((zs <= z) & (z < n - 1))
        def _():
            act(1)

        @pl.when((zs >= z) & (z > 0))
        def _():
            act(0)

    def send_band(k):
        piece = band(k)
        for i in range(1, q_count):
            spot = inc.at[base + i - 1, :, piece]
            pltpu.make_async_copy(spot, spot, part_recv.at[i - 1, k]).wait()
        square = jnp.zeros((piece.size, 1), jnp.float32)
        for c in range(PARTS):
            total = acc[c, piece] + kept[piece, col(c)].astype(jnp.float32)
            for i in range(1, q_count):
                total = total + inc[base + i - 1, c, piece].astype(jnp.float32)
            after = total.astype(jnp.bfloat16)
            kept[piece, col(c)] = after
            after = after.astype(jnp.float32)
            square = square + jnp.sum(after * after, axis=1, keepdims=True)
        norm = lax.rsqrt(square / width + 0.01)
        for c in range(PARTS):
            after = kept[piece, col(c)].astype(jnp.float32)
            toks[z, c, piece] = (after * norm * gain_ref[:, col(c)]).astype(jnp.bfloat16)
        each_side(z, lambda side: token_copy(z, k, side).start())

    for e in range(q_count):
        theirs, ours = spot_of(e, 1 - core), spot_of(e, core)
        if e == 0:
            share_block(3 - opening)
            mate_copy.wait()
        else:
            act_out[theirs] = activate_block(2 * theirs + 1 - core)
            act_copy(theirs).start()
            act_in[ours, core] = activate_block(2 * ours + core)
        pltpu.make_async_copy(act_out.at[ours], act_out.at[ours], act_recv.at[ours]).wait()

        @pl.when(ours != quad)
        def _():
            i = lax.rem(ours - quad + q_count, q_count) - 1
            for c in range(PARTS):
                psend[i, c] = product(ours, c).astype(jnp.bfloat16)
            for k in range(len(BANDS) - 1):
                part_copy(ours, k).start()

        @pl.when(ours == quad)
        def _():
            for c in range(PARTS):
                acc[c] = product(ours, c)

    each_side(z, lambda side: table_copy(z, side).start())
    for k in range(len(BANDS) - 1):
        send_band(k)


    upper = z > n - 1 - z
    middle = (z > 0) & (z < n - 1)

    def arrival(j):
        low = jnp.minimum(z, n - 1 - z)
        out = jnp.where(j <= 2 * low, (j + 1) // 2, j - low)
        down = jnp.where(j <= 2 * low, (j % 2 == 1) == upper, upper)
        return jnp.where(down, z - out, z + out)

    def source(i):
        mine = jnp.where(middle, 0, n - 1)
        return jnp.where(i == mine, z, arrival(jnp.where(middle, i, i + 1)))

    def span(g, index):
        return pl.ds(pl.multiple_of(g * group_rows + index * depth, 16), depth)

    def group(g):
        return pl.ds(g * group_rows, group_rows)

    def exchange(j, g, c, from_ref, to_ref, ss, rs):
        page = lax.rem(j, PAGES)
        side = lax.rem(j, 2)
        for p in range(1, tp):
            other = lax.rem(t + p, tp)
            pltpu.make_async_remote_copy(
                src_ref=from_ref.at[side, c, span(g, other)],
                dst_ref=to_ref.at[page, c, span(g, t)],
                send_sem=ss.at[side],
                recv_sem=rs.at[page, g, c] if to_ref is arr else rs.at[page, c],
                device_id={"tp": other},
                device_id_type=MESH,
            ).start()
        to_ref[page, c, span(g, t)] = from_ref[side, c, span(g, t)]

    def wait_pieces(ref, page, g, c, rs):
        part = ref.at[page, c, pl.ds(0, (tp - 1) * depth)]
        pltpu.make_async_copy(part, part, rs.at[page, g, c]).wait()

    def wait_sent(j, from_ref, ss):
        part = from_ref.at[lax.rem(j, 2), :, pl.ds(0, (tp - 1) * cap)]
        pltpu.make_async_copy(part, part, ss.at[lax.rem(j, 2)]).wait()

    def piece_of(h):
        return pl.ds(h * (rows // SPLIT), rows // SPLIT)

    def sum_copy(zs, c, h, side):
        target = z + 1 if side else z - 1
        slot = jnp.where(target == zs, n, zs) if side else zs
        return pltpu.make_async_remote_copy(
            src_ref=toks.at[zs, c, piece_of(h)],
            dst_ref=inc.at[slot, c, piece_of(h)],
            send_sem=sum_send.at[zs],
            recv_sem=sum_recv.at[slot, c, h],
            device_id={"sp": target},
            device_id_type=MESH,
        )

    def names(zs):
        table = tabs[zs]
        start = (z * slots).astype(jnp.float32)
        row = lax.broadcasted_iota(jnp.int32, (slots, rows), 0)
        place = (
            lax.rem(row, group_rows) // depth * cap + row // group_rows * depth + lax.rem(row, depth)
        )
        place = place.astype(jnp.float32) + start
        return place == table[0:1, :], place == table[1:2, :], table

    def passes_on(zs):
        return ((zs < z) & (z < n - 1)) | ((zs > z) & (z > 0))

    def arrive(zs, k):
        spot = toks.at[zs, :, pl.ds(band(k).start, band(k).size + band(k + 1).size)]
        pltpu.make_async_copy(spot, spot, tok_recv.at[zs, k // 2]).wait()

    def wait_passed(zs, side):
        table_copy(zs, side).wait_send()
        pltpu.make_async_copy(toks.at[zs], toks.at[zs], tok_send.at[side, zs]).wait()

    def hand_on(j):
        zs = arrival(jnp.minimum(j + 1, n - 1))

        @pl.when((j < n - 1) & passes_on(zs))
        def _():
            previous = jnp.where(zs < z, zs + 1, zs - 1)

            @pl.when(previous != z)
            def _():
                each_side(zs, lambda side: wait_passed(previous, side))

            pltpu.make_async_copy(tabs.at[zs], tabs.at[zs], tab_recv.at[zs]).wait()
            each_side(zs, lambda side: table_copy(zs, side).start())
            for k in range(len(BANDS) - 1):
                if k % 2 == 0:
                    arrive(zs, k)
                each_side(zs, lambda side: token_copy(zs, k, side).start())

    def take(j):
        zs = source(j)

        @pl.when((zs != z) & jnp.logical_not(passes_on(zs)))
        def _():
            pltpu.make_async_copy(tabs.at[zs], tabs.at[zs], tab_recv.at[zs]).wait()
            for k in range(0, len(BANDS) - 1, 2):
                arrive(zs, k)

        first, second, _ = names(zs)
        pick = jnp.where(first | second, 1.0, 0.0).astype(jnp.bfloat16)
        side = lax.rem(j, 2)
        for c in range(PARTS):
            comp[side, c] = jnp.dot(
                pick, toks[zs, c], preferred_element_type=jnp.float32
            ).astype(jnp.bfloat16)
            exchange(j, 0, c, comp, arr, piece_send, piece_recv)
        for g in range(1, groups):
            for c in range(PARTS):
                exchange(j, g, c, comp, arr, piece_send, piece_recv)

    def run(j, after_group):
        page = lax.rem(j, PAGES)
        side = lax.rem(j, 2)

        @pl.when(j == 0)
        def _():
            for load in expert_loads:
                load.wait()

        step = 256
        for g in range(groups):
            for c in range(PARTS):
                wait_pieces(arr, page, g, c, piece_recv)
                for f in range(0, hidden_width, step):
                    for to, weights in ((ga, wg), (ua, wu)):
                        value = jnp.dot(
                            arr[page, c, group(g)], weights[col(c), f : f + step],
                            preferred_element_type=jnp.float32,
                        )
                        if c:
                            value = value + to[:, f : f + step]
                        if c < PARTS - 1 or to is ga:
                            to[:, f : f + step] = value
                    if c == PARTS - 1:
                        gate = ga[:, f : f + step]
                        hid[:, f : f + step] = (jax.nn.silu(gate) * value).astype(jnp.bfloat16)
            for c in range(PARTS):
                outs[side, c, group(g)] = jnp.dot(
                    hid[...], wd[:, col(c)], preferred_element_type=jnp.float32
                ).astype(jnp.bfloat16)
                exchange(j, g, c, outs, back, back_send, back_recv)
            after_group(g)
        wait_sent(j, comp, piece_send)

    def merge(j, after_part):
        zs = source(j)
        page = lax.rem(j, PAGES)
        first, second, table = names(zs)
        share = jnp.where(first, table[2:3, :], 0.0) + jnp.where(second, table[3:4, :], 0.0)
        share = share.T
        high = share.astype(jnp.bfloat16)
        rest = (share - high.astype(jnp.float32)).astype(jnp.bfloat16)

        def sent(side):
            @pl.when((zs == (0 if side else n - 1)) & ((zs != z) | jnp.logical_not(middle)))
            def _():
                wait_passed(zs, side)

        each_side(zs, sent)
        for c in range(PARTS):
            part = back.at[page, c, pl.ds(0, (tp - 1) * cap)]
            pltpu.make_async_copy(part, part, back_recv.at[page, c]).wait()
            value = jnp.dot(high, back[page, c], preferred_element_type=jnp.float32) + jnp.dot(
                rest, back[page, c], preferred_element_type=jnp.float32
            )

            @pl.when(zs == z)
            def _():
                acc[c] = value

            @pl.when(zs != z)
            def _():
                toks[zs, c] = value.astype(jnp.bfloat16)

            after_part(zs, c)
        wait_sent(j, outs, back_send)

    def send_sums(zs, c):
        for side in range(2):
            @pl.when((zs > z) & (z == 0) if side else (zs < z) & (z == n - 1))
            def _():
                for h in range(SPLIT):
                    sum_copy(zs, c, h, side).start()

    def relay(turn, p, side):
        zs = turn if side else n - 1 - turn
        c, h = p // SPLIT, p % SPLIT

        @pl.when((z > 0) & (z < turn) if side else (z < n - 1) & (z > n - 1 - turn))
        def _():
            spot = inc.at[zs, c, piece_of(h)]
            pltpu.make_async_copy(spot, spot, sum_recv.at[zs, c, h]).wait()
            toks[zs, c, piece_of(h)] = (
                toks[zs, c, piece_of(h)].astype(jnp.float32)
                + inc[zs, c, piece_of(h)].astype(jnp.float32)
            ).astype(jnp.bfloat16)
            sum_copy(zs, c, h, side).start()

    def relays(turn, start, stop):
        def both(side):
            for p in range(start, stop):
                if p < PARTS * SPLIT:
                    relay(turn, p, side)
                if p >= LAG:
                    relay(turn, p - LAG, 1 - side)

        @pl.when((turn > 0) & upper)
        def _():
            both(0)

        @pl.when((turn > 0) & jnp.logical_not(upper))
        def _():
            both(1)

    def merged(zs, j):
        out = jnp.abs(zs - z)
        low = jnp.minimum(z, n - 1 - z)
        near = jnp.where((zs < z) == upper, 2 * out - 1, 2 * out)
        return jnp.where(out <= low, near, out + low) < j

    def is_early(turn):
        up = (z >= turn) | merged(turn, turn)
        down = (z <= n - 1 - turn) | merged(n - 1 - turn, turn)
        return middle & (turn > 0) & up & down

    pieces = PARTS * SPLIT
    early_stops = (pieces // 8, pieces // 2, pieces + LAG)

    def early_relays(turn, stop):
        start = (0,) + early_stops
        start = start[start.index(stop) - 1]

        @pl.when(is_early(turn))
        def _():
            relays(turn, start, stop)

    def merge_and_relay(j):
        late = jnp.logical_not(is_early(j))

        def after(zs, c):
            @pl.when(late)
            def _():
                relays(j, c * SPLIT, (c + 1) * SPLIT)

        merge(j, after)

        @pl.when(late)
        def _():
            relays(j, pieces, pieces + LAG)

    def body(j, carry):
        ahead = jnp.where(middle, j + 1, j)

        @pl.when((j == 1) & jnp.logical_not(middle))
        def _():
            merge(j - 1, send_sums)

        @pl.when(ahead < n)
        def _():
            take(ahead)

        @pl.when((j > 1) & jnp.logical_not(middle))
        def _():
            merge(j - 1, send_sums)

        @pl.when(j < n)
        def _():
            early_relays(j - 1, early_stops[0])
            run(j, lambda g: early_relays(j - 1, early_stops[min(g + 1, 1)]) if g == 0 else None)
            early_relays(j - 1, early_stops[2])

        @pl.when(j > 0)
        def _():
            hand_on(j + 1)

        @pl.when((j > 0) & middle)
        def _():
            merge_and_relay(j - 1)

        return carry

    @pl.when(middle)
    def _():
        take(0)
        each_side(z, lambda side: wait_passed(z, side))
        pl.semaphore_signal(turn_sem, inc=1, device_id={"tp": mate}, device_id_type=MESH)
        pl.semaphore_wait(turn_sem, 1)
        hand_on(0)
        hand_on(1)

    lax.fori_loop(0, n + 1, body, 0)

    def final(c, h):
        piece = piece_of(h)

        @pl.when(z < n - 1)
        def _():
            spot = inc.at[z, c, piece]
            pltpu.make_async_copy(spot, spot, sum_recv.at[z, c, h]).wait()
            acc[c, piece] = acc[c, piece] + inc[z, c, piece].astype(jnp.float32)

        @pl.when(z > 0)
        def _():
            spot = inc.at[n, c, piece]
            pltpu.make_async_copy(spot, spot, sum_recv.at[n, c, h]).wait()
            acc[c, piece] = acc[c, piece] + inc[n, c, piece].astype(jnp.float32)

        kept[piece, col(c)] = (
            kept[piece, col(c)].astype(jnp.float32) + acc[c, piece]
        ).astype(jnp.bfloat16)

    for c in range(PARTS):
        for h in range(SPLIT):
            final(c, h)

    def drain(zs, carry):
        @pl.when(zs != z)
        def _():
            pltpu.make_async_copy(toks.at[zs], toks.at[zs], sum_send.at[zs]).wait()

        return carry

    lax.fori_loop(0, n, drain, 0)
    others = stats.at[pl.ds(0, tp - 1)]
    pltpu.make_async_copy(others, others, stat_send.at[0]).wait()
    for e in range(q_count):
        act_copy(e).wait_send()
    for i in range(q_count - 1):
        pltpu.make_async_copy(psend.at[i], psend.at[i], part_send.at[i]).wait()

    @pl.when(z < n - 1)
    def _():
        halo_copy(1).wait_send()

    @pl.when(z > 0)
    def _():
        halo_copy(0).wait_send()


def shards(
    latents,
    conv_value,
    conv_gate,
    conv_taps,
    conv_gain,
    point_weight,
    channel_gain,
    expert_ids,
    expert_weights,
    gate_weight,
    up_weight,
    down_weight,
):
    n, tp = lax.axis_size("sp"), lax.axis_size("tp")
    rows, top_count = expert_ids.shape
    experts = gate_weight.shape[0] * n * tp
    cap = -(-(2 * top_count * rows // experts) // 16) * 16
    block, chans = conv_value.shape
    width = latents.shape[1]
    taps_count = conv_taps.shape[0]
    hidden_width = gate_weight.shape[2]
    slots = tp * cap
    groups = 2 if cap % 32 == 0 else 1
    cols = width // PARTS
    edge = -(-(taps_count // 2) // 16) * 16
    q_count = tp // 2
    spots = max(n + 1, 2 * chans // rows + q_count - 1)
    dma = pltpu.SemaphoreType.DMA
    bf16, f32 = jnp.bfloat16, jnp.float32
    hbm = pl.BlockSpec(memory_space=pltpu.HBM)
    vmem = pltpu.VMEM
    scratch = [
        vmem((block, chans), bf16),
        vmem((block, chans), bf16),
        vmem((taps_count, chans), f32),
        vmem((1, chans), f32),
        vmem((1, width), f32),
        vmem((top_count, rows), jnp.int32),
        vmem((top_count, rows), f32),
        vmem((block + 2 * edge, chans), bf16),
        vmem((8, rows // 2 + 2 * edge, chans), f32),
        vmem((tp, rows, chans), f32),
        vmem((tp, tp, 8, rows), f32),
        vmem((q_count, rows, chans), bf16),
        vmem((q_count, 2, rows, chans), bf16),
        vmem((q_count - 1, PARTS, rows, cols), bf16),
        vmem((n, PARTS, rows, cols), bf16),
        vmem((n, 8, rows), f32),
        vmem((2, PARTS, slots, cols), bf16),
        vmem((2, PARTS, slots, cols), bf16),
        vmem((PAGES, PARTS, slots, cols), bf16),
        vmem((PAGES, PARTS, slots, cols), bf16),
        vmem((spots, PARTS, rows, cols), bf16),
        vmem((PARTS, rows, cols), f32),
        vmem((width, hidden_width), bf16),
        vmem((width, hidden_width), bf16),
        vmem((hidden_width, width), bf16),
        vmem((slots // groups, hidden_width), f32),
        vmem((slots // groups, hidden_width), f32),
        vmem((slots // groups, hidden_width), bf16),
        dma((8,)),
        dma((1,)),
        dma((3,)),
        dma((2,)),
        dma((2,)),
        dma((1,)),
        dma((tp,)),
        dma((1,)),
        dma((1,)),
        dma((q_count,)),
        dma((q_count,)),
        dma((q_count - 1,)),
        dma((q_count - 1, len(BANDS) - 1)),
        dma((2, n)),
        dma((n, (len(BANDS) - 1) // 2)),
        dma((2, n)),
        dma((n,)),
        dma((2,)),
        dma((PAGES, groups, PARTS)),
        dma((2,)),
        dma((PAGES, PARTS)),
        dma((n,)),
        dma((n + 1, PARTS, SPLIT)),
        pltpu.SemaphoreType.REGULAR,
    ]
    return pl.pallas_call(
        functools.partial(layer_kernel, n, tp, taps_count, cap),
        out_shape=vmem((rows, width), bf16),
        in_specs=[hbm] * 12,
        out_specs=pl.BlockSpec(memory_space=pltpu.VMEM),
        scratch_shapes=scratch,
        compiler_params=pltpu.CompilerParams(
            collective_id=0, has_side_effects=True, vmem_limit_bytes=67043328 - 4 * rows * width
        ),
        name="layer",
    )(
        conv_value, conv_gate, conv_taps, conv_gain[None, :], point_weight, latents,
        channel_gain[None, :], expert_ids.T, expert_weights.T,
        gate_weight, up_weight, down_weight,
    )


def solution(mesh):
    return jax.shard_map(
        shards,
        mesh=mesh,
        in_specs=(
            P(("grp", "sp", "tp"), None),
            P(("grp", "sp"), "tp"),
            P(("grp", "sp"), "tp"),
            P(None, "tp"),
            P("tp"),
            P("tp", None),
            P(),
            P(("grp", "sp", "tp"), None),
            P(("grp", "sp", "tp"), None),
            P(("sp", "tp"), None, None),
            P(("sp", "tp"), None, None),
            P(("sp", "tp"), None, None),
        ),
        out_specs=P(("grp", "sp", "tp"), None),
        check_vma=False,
    )
```
